32 devices in a mesh: sp: 16 (over z, y, x), tp: 2 (over core).
Axes of the slice: x: 2, y: 2, z: 4, core: 2. Of those that a mesh axis runs over, the one named last changes fastest.
Arguments:
- residual_in: bfloat16 [4096, 2048], P(('sp', 'tp')), may hold values from -6 to 6
- query_lean: bfloat16 [4096, 8, 96], P('sp', 'tp'), may hold values from -60 to 60
- query_broad: bfloat16 [4096, 8, 160], P('sp', 'tp'), may hold values from -60 to 60
- latent: bfloat16 [4096, 256], P('sp'), may hold values from -6 to 6
- rope_key: bfloat16 [4096, 32], P('sp'), may hold values from -8 to 8
- latent_gain: float32 [256], replicated, may hold values from 0.1 to 1.9
- key_up_lean: bfloat16 [256, 8, 64], P(None, 'tp'), may hold values from -0.375 to 0.375
- key_up_broad: bfloat16 [256, 8, 128], P(None, 'tp'), may hold values from -0.375 to 0.375
- value_up_lean: bfloat16 [256, 8, 64], P(None, 'tp'), may hold values from -0.375 to 0.375
- value_up_broad: bfloat16 [256, 8, 128], P(None, 'tp'), may hold values from -0.375 to 0.375
- out_lean: bfloat16 [8, 64, 2048], P('tp'), may hold values from -0.15625 to 0.15625
- out_broad: bfloat16 [8, 128, 2048], P('tp'), may hold values from -0.15625 to 0.15625
- attn_gain: float32 [2048], replicated, may hold values from 0.1 to 1.9
- mlp_gain: float32 [2048], replicated, may hold values from 0.1 to 1.9
- gate_weight: bfloat16 [2048, 2816], P('sp', 'tp'), may hold values from -0.125 to 0.125
- up_weight: bfloat16 [2048, 2816], P('sp', 'tp'), may hold values from -0.125 to 0.125
- down_weight: bfloat16 [2816, 2048], P('tp', 'sp'), may hold values from -0.109375 to 0.109375
Outputs:
- layer_out: bfloat16 [4096, 2048], P(('sp', 'tp'))
The draws below stay inside these ranges and needn't reach their ends.
All inputs are finite; a program needn't handle non-finite values.
Results may differ from the reference program's by a relative error of at most 0.015.
Values may be sent and summed in bfloat16 or wider, within the bound.
A program may use at most 128 MiB of HBM per device.

```python
import math
import jax
import jax.numpy as jnp
from jax import lax

D = 2048
HEADS_A = 8
HEADS_B = 8
NOPE_A = 64
V_A = 64
NOPE_B = 128
V_B = 128
ROPE = 32
KV_RANK = 256
FF = 2816
QK_A = 96
QK_B = 160
TOKENS = 4096
N_TP = 2


def draw_rope_key(key, part):
    base = jax.random.truncated_normal(jax.random.fold_in(key, 1), -4.0, 4.0, (TOKENS, ROPE), jnp.float32)
    return base.astype(jnp.bfloat16)


def draw_query_lean(key, part):
    base = jax.random.truncated_normal(jax.random.fold_in(key, 2), -4.0, 4.0, (TOKENS, HEADS_A, QK_A), jnp.float32)
    return base.astype(jnp.bfloat16)


def draw_query_broad(key, part):
    base = jax.random.truncated_normal(jax.random.fold_in(key, 3), -4.0, 4.0, (TOKENS, HEADS_B, QK_B), jnp.float32)
    return base.astype(jnp.bfloat16)


def levels(key, extent, pieces, smallest, high):
    def one(position, shards_of):
        heights = jax.random.uniform(jax.random.fold_in(jax.random.fold_in(key, 6), position), (shards_of,), jnp.float32, smallest / len(pieces), high / len(pieces))
        return jnp.repeat(jnp.exp(heights), extent[position] // shards_of).reshape((-1,) + (1,) * (len(extent) - position - 1))

    factor_of = one(*pieces[0])
    for cut in pieces[1:]:
        factor_of = factor_of * one(*cut)
    return factor_of


def centred(own_key, extent, scale, bound, cuts=(), held_as=jnp.bfloat16):
    loudness = levels(own_key, extent, cuts, -0.22, 0.18) if cuts else 1.0
    values = jax.random.normal(own_key, extent, jnp.float32) * scale * loudness
    return jnp.minimum(jnp.maximum(values, -bound), bound).astype(held_as)


def setup_inputs(seed: int = 0) -> dict:
    seeds = jax.random.split(jax.random.key(seed), 18)
    return {
        "residual_in": centred(seeds[0], (TOKENS, D), 1.0, 6.0, ((0, 32),)),
        "query_lean": draw_query_lean(jax.random.fold_in(seeds[17], 71), 0),
        "query_broad": draw_query_broad(jax.random.fold_in(seeds[17], 71), 0),
        "latent": centred(seeds[3], (TOKENS, KV_RANK), 1.0, 6.0, ((0, 16),)),
        "rope_key": draw_rope_key(jax.random.fold_in(seeds[17], 71), 0),
        "latent_gain": jnp.clip(1.0 + 0.18 * jax.random.normal(seeds[5], (KV_RANK,), jnp.float32), 0.1, 1.9),
        "key_up_lean": centred(seeds[6], (KV_RANK, HEADS_A, NOPE_A), KV_RANK ** -0.5, 0.375, ((1, 2),)),
        "key_up_broad": centred(seeds[7], (KV_RANK, HEADS_B, NOPE_B), KV_RANK ** -0.5, 0.375, ((1, 2),)),
        "value_up_lean": centred(seeds[8], (KV_RANK, HEADS_A, V_A), KV_RANK ** -0.5, 0.375, ((1, 2),)),
        "value_up_broad": centred(seeds[9], (KV_RANK, HEADS_B, V_B), KV_RANK ** -0.5, 0.375, ((1, 2),)),
        "out_lean": centred(seeds[10], (HEADS_A, V_A, D), (HEADS_A * V_A + HEADS_B * V_B) ** -0.5, 0.15625, ((0, 2),)),
        "out_broad": centred(seeds[11], (HEADS_B, V_B, D), (HEADS_A * V_A + HEADS_B * V_B) ** -0.5, 0.15625, ((0, 2),)),
        "attn_gain": jnp.clip(1.0 + 0.18 * jax.random.normal(seeds[12], (D,), jnp.float32), 0.1, 1.9),
        "mlp_gain": jnp.clip(1.0 + 0.18 * jax.random.normal(seeds[13], (D,), jnp.float32), 0.1, 1.9),
        "gate_weight": centred(seeds[14], (D, FF), D ** -0.5, 0.125, ((0, 16), (1, 2))),
        "up_weight": centred(seeds[15], (D, FF), D ** -0.5, 0.125, ((0, 16), (1, 2))),
        "down_weight": centred(seeds[16], (FF, D), FF ** -0.5, 0.109375, ((0, 2), (1, 16))),
    }


THETA = 10000.0
EPS = 1e-06
NEGATIVE = -1e+30

def rotate(values, positions):
    width = values.shape[-1]
    half = width // 2
    freqs = THETA ** (-2.0 * jnp.arange(half, dtype=jnp.float32) / width)
    angle = positions.astype(jnp.float32)[:, None] * freqs[None, :]
    cosine = jnp.cos(angle)
    sine = jnp.sin(angle)
    if values.ndim == 3:
        cosine = cosine[:, None, :]
        sine = sine[:, None, :]
    first = values[..., :half]
    second = values[..., half:]
    return jnp.concatenate([first * cosine - second * sine, first * sine + second * cosine], axis=-1)

def normalize(values, gain):
    return values * lax.rsqrt(lax.optimization_barrier(jnp.mean(values * values, axis=-1, keepdims=True)) + EPS) * gain.astype(jnp.float32)

def widen(values):
    return lax.optimization_barrier(values).astype(jnp.float32)

def attend_group(query, key_up, value_up, latent_normed, rotated_key, positions):
    nope = key_up.shape[2]
    heads = key_up.shape[1]
    vsize = value_up.shape[2]
    scale = query.shape[2] ** (-0.5)
    lat = latent_normed.astype(jnp.float32)
    keys = widen(jnp.einsum('kr,rhd->khd', lat, key_up.astype(jnp.float32)).astype(jnp.bfloat16))
    values = widen(jnp.einsum('kr,rhd->khd', lat, value_up.astype(jnp.float32)).astype(jnp.bfloat16))
    rot_keys = rotated_key.astype(jnp.float32)
    query_nope = query[:, :, :nope].astype(jnp.float32)
    query_rot = widen(rotate(query[:, :, nope:].astype(jnp.float32), positions).astype(jnp.bfloat16))
    size = math.gcd(TOKENS, 256)

    def block(index):
        start = (index * size).astype(jnp.int32)
        rows = start + jnp.arange(size, dtype=jnp.int32)
        part_nope = lax.dynamic_slice_in_dim(query_nope, start, size, 0)
        part_rot = lax.dynamic_slice_in_dim(query_rot, start, size, 0)
        scores = (jnp.einsum('qhd,khd->hqk', part_nope, keys) + jnp.einsum('qhr,kr->hqk', part_rot, rot_keys)) * scale
        visible = positions[None, :] <= rows[:, None]
        scores = jnp.where(visible[None], scores, NEGATIVE)
        peak = lax.optimization_barrier(jnp.max(scores, axis=-1, keepdims=True))
        weights = jnp.where(visible[None], jnp.exp(scores - peak), 0.0)
        total = lax.optimization_barrier(jnp.sum(weights, axis=-1))
        rounded = widen(weights.astype(jnp.bfloat16))
        result = jnp.einsum('hqk,khv->qhv', rounded, values) / jnp.transpose(total)[:, :, None]
        return result.astype(jnp.bfloat16)
    blocks = lax.map(block, jnp.arange(TOKENS // size, dtype=jnp.int32))
    return blocks.reshape(TOKENS, heads, vsize)

def reference(residual_in, query_lean, query_broad, latent, rope_key, latent_gain, key_up_lean, key_up_broad, value_up_lean, value_up_broad, out_lean, out_broad, attn_gain, mlp_gain, gate_weight, up_weight, down_weight):
    positions = jnp.arange(TOKENS, dtype=jnp.int32)
    latent_normed = normalize(latent.astype(jnp.float32), latent_gain).astype(jnp.bfloat16)
    rotated_key = rotate(rope_key.astype(jnp.float32), positions).astype(jnp.bfloat16)
    attended_lean = attend_group(query_lean, key_up_lean, value_up_lean, latent_normed, rotated_key, positions)
    attended_broad = attend_group(query_broad, key_up_broad, value_up_broad, latent_normed, rotated_key, positions)
    lean_per = HEADS_A // N_TP
    broad_per = HEADS_B // N_TP
    head_sum = jnp.zeros((TOKENS, D), jnp.float32)
    for group in range(N_TP):
        partial_value = jnp.einsum('qhv,hvd->qd', attended_lean[:, group * lean_per:(group + 1) * lean_per].astype(jnp.float32), out_lean[group * lean_per:(group + 1) * lean_per].astype(jnp.float32))
        partial_value = partial_value + jnp.einsum('qhv,hvd->qd', attended_broad[:, group * broad_per:(group + 1) * broad_per].astype(jnp.float32), out_broad[group * broad_per:(group + 1) * broad_per].astype(jnp.float32))
        head_sum = head_sum + partial_value.astype(jnp.bfloat16).astype(jnp.float32)
    branch = normalize(head_sum, attn_gain)
    mixed = (residual_in.astype(jnp.float32) + branch).astype(jnp.bfloat16)
    normed = normalize(mixed.astype(jnp.float32), mlp_gain).astype(jnp.bfloat16)
    gate = jnp.dot(normed, gate_weight, preferred_element_type=jnp.float32)
    up = jnp.dot(normed, up_weight, preferred_element_type=jnp.float32)
    hidden = (jax.nn.silu(gate) * up).astype(jnp.bfloat16)
    units = FF // N_TP
    channel_sum = jnp.zeros((TOKENS, D), jnp.float32)
    for group in range(N_TP):
        partial_value = jnp.dot(hidden[:, group * units:(group + 1) * units], down_weight[group * units:(group + 1) * units], preferred_element_type=jnp.float32)
        channel_sum = channel_sum + partial_value.astype(jnp.bfloat16).astype(jnp.float32)
    return (mixed.astype(jnp.float32) + 0.5 * channel_sum).astype(jnp.bfloat16)
```

```python
import functools
import math

import jax
import jax.numpy as jnp
from jax import lax
from jax.experimental import pallas as pl
from jax.experimental.pallas import tpu as pltpu
from jax.sharding import PartitionSpec as P

THETA = 10000.0
EPS = 1e-06
NEGATIVE = -1e30


def rotate(values, positions):
    width = values.shape[-1]
    half = width // 2
    freqs = THETA ** (-2.0 * jnp.arange(half, dtype=jnp.float32) / width)
    angle = positions.astype(jnp.float32)[:, None] * freqs[None, :]
    cosine = jnp.cos(angle)
    sine = jnp.sin(angle)
    if values.ndim == 3:
        cosine = cosine[:, None, :]
        sine = sine[:, None, :]
    first = values[..., :half]
    second = values[..., half:]
    return jnp.concatenate(
        [first * cosine - second * sine, first * sine + second * cosine], axis=-1
    )


def normalize(values, gain):
    return values * lax.rsqrt(jnp.mean(values * values, axis=-1, keepdims=True) + EPS) * gain


def block_keys(weights, latent_rows):
    projected = []
    for key_up, value_up in weights:
        keys = jnp.einsum(
            "kr,rhd->khd", latent_rows, key_up, preferred_element_type=jnp.float32
        ).astype(jnp.bfloat16)
        values = jnp.einsum(
            "kr,rhd->khd", latent_rows, value_up, preferred_element_type=jnp.float32
        ).astype(jnp.bfloat16)
        projected.append((keys, values))
    return projected


def attend(carry, queries, projected, rotated_rows, key_pos, query_pos):
    updated = []
    visible = key_pos[None, :] <= query_pos[:, None]
    for state, query, pair in zip(carry, queries, projected):
        query_nope, query_rot, scale = query
        keys, values = pair
        peak, total, accum = state
        scores = (
            jnp.einsum("qhd,khd->hqk", query_nope, keys, preferred_element_type=jnp.float32)
            + jnp.einsum("qhr,kr->hqk", query_rot, rotated_rows, preferred_element_type=jnp.float32)
        ) * scale
        scores = jnp.where(visible[None], scores, NEGATIVE)
        new_peak = jnp.maximum(peak, jnp.max(scores, axis=-1))
        weights = jnp.where(visible[None], jnp.exp(scores - new_peak[..., None]), 0.0)
        factor = jnp.exp(peak - new_peak)
        total = total * factor + jnp.sum(weights, axis=-1)
        accum = accum * factor[..., None] + jnp.einsum(
            "hqk,khv->hqv", weights.astype(jnp.bfloat16), values, preferred_element_type=jnp.float32
        )
        updated.append((new_peak, total, accum))
    return tuple(updated)


def fold_piece(carry, latent_piece, rotated_piece, piece_pos, weights, segments):
    count = latent_piece.shape[0]
    block = math.gcd(count, 1024)
    last_all = segments[0][1][-1]

    def one_block(index, state):
        lat_rows = lax.dynamic_slice_in_dim(latent_piece, index * block, block, 0)
        rot_rows = lax.dynamic_slice_in_dim(rotated_piece, index * block, block, 0)
        pos_rows = lax.dynamic_slice_in_dim(piece_pos, index * block, block, 0)
        first_key = jnp.min(pos_rows)

        def work(inner):
            projected = block_keys(weights, lat_rows)
            results = []
            for inner_seg, segment in zip(inner, segments):
                queries, seg_pos = segment
                results.append(
                    lax.cond(
                        first_key <= seg_pos[-1],
                        lambda held, queries=queries, seg_pos=seg_pos: attend(
                            held, queries, projected, rot_rows, pos_rows, seg_pos
                        ),
                        lambda held: held,
                        inner_seg,
                    )
                )
            return tuple(results)

        return lax.cond(first_key <= last_all, work, lambda inner: inner, state)

    return lax.fori_loop(0, count // block, one_block, carry)


def shards(
    residual_in,
    query_lean,
    query_broad,
    latent,
    rope_key,
    latent_gain,
    key_up_lean,
    key_up_broad,
    value_up_lean,
    value_up_broad,
    out_lean,
    out_broad,
    attn_gain,
    mlp_gain,
    gate_weight,
    up_weight,
    down_weight,
):
    tokens_here = query_lean.shape[0]
    n_tp = lax.axis_size("tp")
    share = tokens_here // n_tp
    sp_index = lax.axis_index("sp")
    first = sp_index * tokens_here
    query_pos = first + jnp.arange(tokens_here, dtype=jnp.int32)
    rope_width = rope_key.shape[1]
    weights = ((key_up_lean, value_up_lean), (key_up_broad, value_up_broad))
    segment_rows = (query_lean, query_broad, query_pos)
    segments = []
    initial = []
    lean_rows, broad_rows, seg_pos = segment_rows
    queries = []
    states = []
    for query, value_up in ((lean_rows, value_up_lean), (broad_rows, value_up_broad)):
        nope = query.shape[2] - rope_width
        query_rot = rotate(query[:, :, nope:].astype(jnp.float32), seg_pos).astype(jnp.bfloat16)
        queries.append((query[:, :, :nope], query_rot, query.shape[2] ** (-0.5)))
        heads = query.shape[1]
        rows = query.shape[0]
        states.append(
            (
                jnp.full((heads, rows), NEGATIVE, jnp.float32),
                jnp.zeros((heads, rows), jnp.float32),
                jnp.zeros((heads, rows, value_up.shape[2]), jnp.float32),
            )
        )
    segments.append((tuple(queries), seg_pos))
    initial.append(tuple(states))
    segments = tuple(segments)
    initial = tuple(initial)
    sent_latent = normalize(latent.astype(jnp.float32), latent_gain).astype(jnp.bfloat16)
    sent_rot = rotate(rope_key.astype(jnp.float32), query_pos).astype(jnp.bfloat16)
    pieces = (
        lax.all_gather(sent_latent, "sp", axis=0, tiled=True),
        lax.all_gather(sent_rot, "sp", axis=0, tiled=True),
    )
    piece_pos = jnp.arange(pieces[0].shape[0], dtype=jnp.int32)
    folded = fold_piece(initial, pieces[0], pieces[1], piece_pos, weights, segments)
    results = [
        [(accum / total[..., None]).astype(jnp.bfloat16) for peak, total, accum in seg_state]
        for seg_state in folded
    ]
    attended = results[0]
    term = jnp.zeros((share * lax.axis_size("tp"), out_lean.shape[2]), jnp.float32)
    for rows_all, weight in ((attended[0], out_lean), (attended[1], out_broad)):
        rows = rows_all
        term = term + jnp.einsum("hqv,hvd->qd", rows, weight, preferred_element_type=jnp.float32)
    head_sum = lax.psum_scatter(
        term.astype(jnp.bfloat16), "tp", scatter_dimension=0, tiled=True
    ).astype(jnp.float32)
    branch = normalize(head_sum, attn_gain)
    kept = (residual_in.astype(jnp.float32) + branch).astype(jnp.bfloat16)
    normed = normalize(kept.astype(jnp.float32), mlp_gain).astype(jnp.bfloat16)
    whole_normed = lax.all_gather(normed, "tp", axis=0, tiled=True)
    gate_whole, up_whole, down_whole = (
        lax.all_gather(gate_weight, "sp", axis=0, tiled=True),
        lax.all_gather(up_weight, "sp", axis=0, tiled=True),
        lax.all_gather(down_weight, "sp", axis=1, tiled=True),
    )
    gate = jnp.dot(whole_normed, gate_whole, preferred_element_type=jnp.float32)
    up = jnp.dot(whole_normed, up_whole, preferred_element_type=jnp.float32)
    hidden = (jax.nn.silu(gate) * up).astype(jnp.bfloat16)
    rows = hidden
    channel_sum = lax.psum_scatter(
        jnp.dot(rows, down_whole, preferred_element_type=jnp.float32).astype(jnp.bfloat16),
        "tp",
        scatter_dimension=0,
        tiled=True,
    ).astype(jnp.float32)
    return (kept.astype(jnp.float32) + 0.5 * channel_sum).astype(jnp.bfloat16)


LOG2E = math.log2(math.e)


def grid_of(mesh):
    n_sp, n_tp = mesh.shape["sp"], mesh.shape["tp"]
    devices = mesh.devices.reshape(n_sp, n_tp)
    try:
        places = [tuple(device.coords) for device in devices[:, 0]]
        partners = [tuple(device.coords) for device in devices[:, -1]]
    except Exception:
        return (n_sp // 4, 2, 2) if n_sp % 4 == 0 else None
    if places != partners:
        return None
    low = [min(place[k] for place in places) for k in range(3)]
    sizes = [max(place[k] for place in places) - low[k] + 1 for k in range(3)]
    wide_z, wide_y, wide_x = sizes[2], sizes[1], sizes[0]
    if wide_z * wide_y * wide_x != n_sp:
        return None
    for index, place in enumerate(places):
        x, y, z = (place[k] - low[k] for k in range(3))
        if (z * wide_y + y) * wide_x + x != index:
            return None
    return wide_z, wide_y, wide_x


def hop_table(grid, past):
    wide_z = grid[0]
    entries = [
        (dz, fy, fx)
        for dz in range(1 - wide_z, 1 if past else wide_z)
        for fy in range(2)
        for fx in range(2)
        if (dz, fy, fx) != (0, 0, 0)
    ]
    entries.sort(key=lambda e: (abs(e[0]) + e[1] + e[2], abs(e[0]), e))
    return entries


def layer_kernel(
    grid, shapes, res_in, qlt, qbt, lat, cosine, sine, ag, mg, kul, kub, vul, vub, wol_in, wob_in, gw, uw, dw, out,
    lat_all, gate_all, up_all, down_all, ext_all, own_g, own_u, own_d, own_e, ql, qb, ktl, ktb, valt_l, valt_b,
    peak, total, acc_l, acc_b, att, term, inbox, kept, rows_all, hidden, inbox2, psum, inbox3, wol, wob, res,
    lat_recv, lat_send, lat_pair, recv, send, own_sem, pair_send, pair_recv,
):
    wide_z, wide_y, wide_x = grid
    n_sp = wide_z * wide_y * wide_x
    tokens, share, rope = shapes
    heads_l, heads_b = qlt.shape[0], qbt.shape[0]
    bf16, f32 = jnp.bfloat16, jnp.float32
    me = lax.axis_index("sp")
    core = lax.axis_index("tp")
    my_x = lax.rem(me, wide_x)
    my_y = lax.rem(me // wide_x, wide_y)
    my_z = me // (wide_x * wide_y)
    layer = wide_y * wide_x
    flip_y = me + (1 - 2 * my_y) * wide_x
    flip_x = me + (1 - 2 * my_x)
    side = lax.rem(my_z, 2)
    partner = me + (1 - 2 * side) * layer
    z_ways = [
        (step, my_z + step < wide_z if step > 0 else my_z + step >= 0,
         jnp.clip(me + step * layer, 0, n_sp - 1))
        for step in (1, -1, 2, -2)
    ]

    def z_way(step):
        return next(way for way in z_ways if way[0] == step)

    def run(condition, action):
        pl.when(condition)(action)

    gate_rows, units = gw.shape
    down_cols = dw.shape[1]
    main = gate_all.shape[1]
    extra = units - 2 * main
    fetch = [
        pltpu.make_async_copy(src, dst, own_sem.at[k])
        for k, (src, dst) in enumerate((
            (gw, own_g), (uw, own_u), (dw, own_d),
            (gw.at[:, pl.ds(2 * main, extra)], own_e.at[0]),
            (uw.at[:, pl.ds(2 * main, extra)], own_e.at[1]),
            (dw.at[pl.ds(2 * main, extra), :], own_e.at[2]),
            (wol_in, wol), (wob_in, wob), (res_in, res),
        ))
    ]
    lat_rows = lat.shape[0]
    own_lat = pltpu.make_async_copy(
        lat, lat_all.at[pl.ds(pl.multiple_of(me * lat_rows, lat_rows), lat_rows)], own_sem.at[len(fetch)]
    )
    for copy in fetch:
        copy.start()
    own_lat.start()

    barrier = pltpu.get_barrier_semaphore()
    for where in (flip_x, flip_y):
        pl.semaphore_signal(barrier, inc=1, device_id={"sp": where})
    pl.semaphore_signal(barrier, inc=1, device_id={"tp": 1 - core})
    greeted = 3
    for _, exists, where in z_ways:
        run(exists, lambda where=where: pl.semaphore_signal(barrier, inc=1, device_id={"sp": where}))
        greeted = greeted + jnp.where(exists, 1, 0)
    pl.semaphore_wait(barrier, greeted)

    half = lat_rows // 2
    first = pl.multiple_of(core * half, 16)

    def lat_at(i):
        return lat_all.at[pl.ds(pl.multiple_of(i * lat_rows + first, 16), half)]

    def lat_copy(i, mine, where):
        return pltpu.make_async_remote_copy(
            src_ref=lat.at[pl.ds(first, half)] if mine else lat_at(i), dst_ref=lat_at(i),
            send_sem=lat_send.at[0], recv_sem=lat_recv.at[i], device_id={"sp": where},
        )

    def pair_lat(i):
        return pltpu.make_async_remote_copy(
            src_ref=lat_at(i), dst_ref=lat_at(i), send_sem=lat_send.at[1],
            recv_sem=lat_pair.at[i], device_id={"tp": 1 - core},
        )

    def lat_forward(i, fy, fx, mine):
        column = jnp.logical_and(fy == 0, fx == 0)
        up = z_way(1)
        run(jnp.logical_and(column, up[1]), lambda: lat_copy(i, mine, up[2]).start())
        to_x = jnp.logical_or(column, jnp.logical_and(core == 1, jnp.logical_and(fy == 1, fx == 0)))
        to_y = jnp.logical_or(column, jnp.logical_and(core == 0, jnp.logical_and(fy == 0, fx == 1)))
        run(to_x, lambda: lat_copy(i, mine, flip_x).start())
        run(to_y, lambda: lat_copy(i, mine, flip_y).start())

    lat_forward(me, my_y * 0, my_x * 0, True)

    per = 4

    def words_of(table):
        codes = [((dz + wide_z - 1) * 2 + fy) * 2 + fx for dz, fy, fx in table]
        return [
            sum(code << (7 * k) for k, code in enumerate(codes[at:at + per]))
            for at in range(0, len(codes), per)
        ]

    def origin_of(n, words):
        word = jnp.int32(words[0])
        for k in range(1, len(words)):
            word = jnp.where(n // per == k, jnp.int32(words[k]), word)
        rem = lax.rem(n, per)
        for k in range(1, per):
            word = jnp.where(rem >= k, word // 128, word)
        code = lax.rem(word, 128)
        return code // 4 - (wide_z - 1), lax.rem(code // 2, 2), lax.rem(code, 2)

    def index_of(dz, fy, fx):
        oy = my_y + fy * (1 - 2 * my_y)
        ox = my_x + fx * (1 - 2 * my_x)
        return ((my_z + dz) * wide_y + oy) * wide_x + ox

    past = hop_table(grid, True)
    past_words = words_of(past)

    def lat_event(n, _):
        dz, fy, fx = origin_of(n, past_words)

        @pl.when(my_z + dz >= 0)
        def _():
            i = index_of(dz, fy, fx)
            lat_copy(i, False, flip_x).wait_recv()
            lat_forward(i, fy, fx, False)
            pair_lat(i).start()

        return 0

    lax.fori_loop(0, len(past), lat_event, 0)

    def slot_at(ref, i):
        return ref.at[pl.ds(pl.multiple_of(i * gate_rows, gate_rows), gate_rows)]

    def down_slot(dz, fy, fx):
        slot = (fy * 2 + fx) * wide_z + my_z + dz
        return down_all.at[pl.ds(0, main), pl.ds(pl.multiple_of(slot * down_cols, down_cols), down_cols)]

    def place(p, dz, fy, fx):
        i = index_of(dz, fy, fx)
        if p == 0:
            return slot_at(gate_all, i)
        if p == 1:
            return slot_at(up_all, i)
        if p == 2:
            return down_slot(dz, fy, fx)
        return ext_all.at[i]

    def own_half(p, h):
        lanes = pl.ds(pl.multiple_of(h * main, extra), main)
        if p == 0:
            return own_g.at[:, lanes]
        if p == 1:
            return own_u.at[:, lanes]
        if p == 2:
            return own_d.at[lanes, :]
        return own_e

    def part_copy(p, src, dst, i, where):
        return pltpu.make_async_remote_copy(
            src_ref=src, dst_ref=dst, send_sem=send.at[p], recv_sem=recv.at[p, i], device_id={"sp": where},
        )

    has_extra = core == side
    x_first = (True, False, core == 0, False)

    def to_z(p, src, step, origin, i, condition=True):
        _, exists, where = z_way(step)
        dst = place(p, *origin) if p == 2 else place(p, *origin)
        run(jnp.logical_and(exists, condition), lambda: part_copy(p, src, dst, i, where).start())

    def seen(origin, fy, fx):
        return origin[0], origin[1] + fy - 2 * origin[1] * fy, origin[2] + fx - 2 * origin[2] * fx

    def dst_for(p, origin, fy, fx):
        if p == 2:
            return down_slot(*seen(origin, fy, fx))
        return place(p, *origin)

    def send_own(p):
        here = (0, 0, 0)
        mine = own_half(p, side)
        other = own_half(p, 1 - side)
        same = has_extra if p == 3 else True
        cross = jnp.logical_not(has_extra) if p == 3 else True
        for step in (1, -1):
            to_z(p, other, step, here, me, cross)
        for step in (2, -2):
            to_z(p, mine, step, here, me, same)

        def flips():
            part_copy(p, mine, dst_for(p, here, 0, 1), me, flip_x).start()
            part_copy(p, mine, dst_for(p, here, 1, 0), me, flip_y).start()

        if p == 3:
            run(has_extra, flips)
        else:
            flips()

    def part_event(p, dz, fy, fx):
        origin = (dz, fy, fx)
        i = index_of(*origin)
        here = place(p, *origin)
        part_copy(p, here, here, i, flip_x).wait_recv()
        column = jnp.logical_and(fy == 0, fx == 0)
        to_z(p, here, 2, origin, i, jnp.logical_and(column, dz < 0))
        to_z(p, here, -2, origin, i, jnp.logical_and(column, dz > 0))
        x_line = jnp.logical_and(fy == 0, fx == 1)
        y_line = jnp.logical_and(fy == 1, fx == 0)
        if x_first[p] is True:
            to_x, to_y = column, jnp.logical_or(column, x_line)
        elif x_first[p] is False:
            to_x, to_y = jnp.logical_or(column, y_line), column
        else:
            to_x = jnp.logical_or(column, jnp.logical_and(y_line, jnp.logical_not(x_first[p])))
            to_y = jnp.logical_or(column, jnp.logical_and(x_line, x_first[p]))
        run(to_x, lambda: part_copy(p, here, dst_for(p, origin, 0, 1), i, flip_x).start())
        run(to_y, lambda: part_copy(p, here, dst_for(p, origin, 1, 0), i, flip_y).start())

    for copy in fetch[:6]:
        copy.wait()
    for p in (0, 1, 3):
        send_own(p)

    whole = hop_table(grid, False)
    whole_words = words_of(whole)

    def gate_event(n, _):
        dz, fy, fx = origin_of(n, whole_words)

        @pl.when(jnp.logical_and(my_z + dz >= 0, my_z + dz < wide_z))
        def _():
            part_event(0, dz, fy, fx)
            part_event(1, dz, fy, fx)
            run(has_extra, lambda: part_event(3, dz, fy, fx))

        return 0

    def down_group(fy, fx):
        def body(t, _):
            dz = jnp.where(lax.rem(t, 2) == 1, -((t + 1) // 2), t // 2)
            ok = jnp.logical_and(my_z + dz >= 0, my_z + dz < wide_z)
            if (fy, fx) == (0, 0):
                ok = jnp.logical_and(ok, dz != 0)
            run(ok, lambda: part_event(2, dz, jnp.int32(fy), jnp.int32(fx)))
            return 0

        lax.fori_loop(0, 2 * wide_z - 1, body, 0)

    own_rows = pl.ds(pl.multiple_of(me * gate_rows, gate_rows), gate_rows)
    own_lanes = pl.ds(pl.multiple_of(side * main, extra), main)
    gate_all[own_rows, :] = own_g[:, own_lanes]
    up_all[own_rows, :] = own_u[:, own_lanes]
    down_all[:main, pl.ds(pl.multiple_of(my_z * down_cols, down_cols), down_cols)] = own_d[own_lanes, :]
    ext_all[me] = own_e[...]

    half_rope = rope // 2
    for given, query in ((qlt, ql), (qbt, qb)):
        nope = given.shape[1] - rope
        for h in range(given.shape[0]):
            one = given[h, nope:nope + half_rope, :].astype(f32)
            two = given[h, nope + half_rope:, :].astype(f32)
            query[h, :nope, :] = given[h, :nope, :]
            query[h, nope:nope + half_rope, :] = (one * cosine[...] - two * sine[...]).astype(bf16)
            query[h, nope + half_rope:, :] = (one * sine[...] + two * cosine[...]).astype(bf16)
    own_lat.wait()

    def lat_arrived(i, _):
        ours = jnp.logical_and(i != me, i < (my_z + 1) * layer)
        run(ours, lambda: pair_lat(i).wait_recv())
        return 0

    lax.fori_loop(0, n_sp, lat_arrived, 0)

    peak[...] = jnp.full(peak.shape, NEGATIVE, f32)
    total[...] = jnp.zeros(total.shape, f32)
    acc_l[...] = jnp.zeros(acc_l.shape, f32)
    acc_b[...] = jnp.zeros(acc_b.shape, f32)
    wide_l = kul.shape[0] // heads_l
    wide_b = kub.shape[0] // heads_b
    contract = (((1,), (1,)), ((), ()))
    contract_rows = (((0,), (0,)), ((), ()))

    def attend_block(j, masked):
        at_j = pl.multiple_of(j * lat_rows, 16)
        rows = lat_all[pl.ds(at_j, tokens), :]
        rot = lat_all[pl.ds(pl.multiple_of(at_j + tokens, 16), rope), :]
        for ups, keys, heads, wide in ((kul, ktl, heads_l, wide_l), (kub, ktb, heads_b, wide_b)):
            made = lax.dot_general(ups[...], rows, contract, preferred_element_type=f32).astype(bf16)
            for h in range(heads):
                keys[h, :wide, :] = made[h * wide:(h + 1) * wide]
                keys[h, wide:, :] = rot
        for ups, held in ((vul, valt_l), (vub, valt_b)):
            held[...] = lax.dot_general(
                ups[...], rows, contract, preferred_element_type=f32
            ).astype(bf16)
        if masked:
            key_pos = lax.broadcasted_iota(jnp.int32, (tokens, tokens), 0)
            visible = key_pos <= lax.broadcasted_iota(jnp.int32, (tokens, tokens), 1)
        for g in range(heads_l + heads_b):
            if g < heads_l:
                h, query, keys, held, acc, wide = g, ql, ktl, valt_l, acc_l, wide_l
            else:
                h, query, keys, held, acc, wide = g - heads_l, qb, ktb, valt_b, acc_b, wide_b
            scores = lax.dot_general(
                keys[h], query[h], contract_rows, preferred_element_type=f32
            ) * (LOG2E * query.shape[1] ** (-0.5))
            if masked:
                scores = jnp.where(visible, scores, NEGATIVE)
            old = peak[g]
            new = jnp.maximum(old, jnp.max(scores, axis=0, keepdims=True))
            weights = jnp.exp2(scores - new)
            factor = jnp.exp2(old - new)
            peak[g] = new
            total[g] = total[g] * factor + jnp.sum(weights, axis=0, keepdims=True)
            acc[h] = acc[h] * factor + jnp.dot(
                held[h * wide:(h + 1) * wide, :], weights.astype(bf16), preferred_element_type=f32
            )

    def step(j, _):
        lax.fori_loop((j * early) // n_sp, ((j + 1) * early) // n_sp, gate_event, 0)
        pl.when(j < me)(lambda: attend_block(j, False))
        return 0

    count = len(whole)
    early = sum(1 for dz, fy, fx in whole if abs(dz) + fy + fx <= 2)
    lax.fori_loop(0, n_sp, step, 0)
    attend_block(me, True)
    send_own(2)
    lax.fori_loop(early, count, gate_event, 0)

    split = heads_l * wide_l
    for heads, wide, acc, base, col in (
        (heads_l, wide_l, acc_l, 0, 0), (heads_b, wide_b, acc_b, heads_l, split),
    ):
        together = wide_b // wide
        for h in range(0, heads, together):
            done = jnp.concatenate(
                [acc[h + k] / total[base + h + k] for k in range(together)], axis=0
            )
            att[:, col + h * wide:col + (h + together) * wide] = done.T.astype(bf16)

    features = out.shape[1]
    block = math.gcd(features, 512)

    for copy in fetch[6:]:
        copy.wait()

    def project(n, _):
        cols = pl.ds(pl.multiple_of(n * block, block), block)
        term[:tokens, cols] = (
            jnp.dot(att[:, :split], wol[:, cols], preferred_element_type=f32)
            + jnp.dot(att[:, split:], wob[:, cols], preferred_element_type=f32)
        ).astype(bf16)
        return 0

    lax.fori_loop(0, features // block, project, 0)
    theirs = pl.ds(pl.multiple_of((1 - core) * share, share), share)

    def to_pair(k, src, dst):
        return pltpu.make_async_remote_copy(
            src_ref=src, dst_ref=dst, send_sem=pair_send.at[k], recv_sem=pair_recv.at[k],
            device_id={"tp": 1 - core},
        )

    def to_partner(k, src, dst):
        return pltpu.make_async_remote_copy(
            src_ref=src, dst_ref=dst, send_sem=pair_send.at[k], recv_sem=pair_recv.at[k],
            device_id={"sp": partner},
        )

    def place_of(of_core, of_side):
        return pl.ds(pl.multiple_of((of_core * 2 + of_side) * share, share), share)

    heads_out = to_pair(0, term.at[theirs], inbox)
    heads_out.start()
    heads_out.wait_recv()
    rows_at_once = math.gcd(share, 16)

    def norms(n, _):
        rows = pl.ds(pl.multiple_of(n * rows_at_once, rows_at_once), rows_at_once)
        full = pl.ds(pl.multiple_of(core * share + n * rows_at_once, rows_at_once), rows_at_once)
        spot = pl.ds(pl.multiple_of((core * 2 + side) * share + n * rows_at_once, rows_at_once), rows_at_once)
        summed = term[full, :].astype(f32) + inbox[rows, :].astype(f32)
        branch = normalize(summed, ag[...])
        mixed = (res[rows, :].astype(f32) + branch).astype(bf16)
        kept[rows, :] = mixed
        rows_all[spot, :] = normalize(mixed.astype(f32), mg[...]).astype(bf16)
        return 0

    lax.fori_loop(0, share // rows_at_once, norms, 0)
    mine_at = rows_all.at[place_of(core, side)]
    rows_out = to_pair(1, mine_at, mine_at)
    rows_far = to_partner(2, mine_at, mine_at)
    rows_out.start()
    rows_far.start()
    heads_out.wait_send()
    far_at = rows_all.at[place_of(core, 1 - side)]
    to_partner(2, far_at, far_at).wait_recv()
    rows_on = to_pair(3, far_at, far_at)
    rows_on.start()
    near_at = rows_all.at[place_of(1 - core, side)]
    to_pair(1, near_at, near_at).wait_recv()
    last_at = rows_all.at[place_of(1 - core, 1 - side)]
    to_pair(3, last_at, last_at).wait_recv()
    down_group(0, 0)

    def feed_from(rows, gate_w, up_w, cols):
        gate = jnp.dot(rows_all[rows, :], gate_w, preferred_element_type=f32)
        up = jnp.dot(rows_all[rows, :], up_w, preferred_element_type=f32)
        hidden[rows, cols] = (gate / (1.0 + jnp.exp(-gate)) * up).astype(bf16)

    span = math.gcd(main, 256)
    chunks = main // span
    group = 2 * tokens // 2

    def group_rows(n):
        return pl.ds(pl.multiple_of(n * group, group), group)

    def feed_loop(n, _):
        rows = group_rows(n // chunks)
        cols = pl.ds(pl.multiple_of(lax.rem(n, chunks) * span, span), span)
        feed_from(rows, gate_all[:, cols], up_all[:, cols], cols)
        return 0

    lax.fori_loop(0, 2 * chunks, feed_loop, 0)

    @pl.when(has_extra)
    def _():
        def body(n, _):
            gate_e = ext_all[:, 0].reshape(n_sp * gate_rows, extra)
            up_e = ext_all[:, 1].reshape(n_sp * gate_rows, extra)
            feed_from(group_rows(n), gate_e, up_e, pl.ds(main, extra))
            return 0

        lax.fori_loop(0, 2, body, 0)

        def lay(i, _):
            oz = i // layer
            fy = jnp.abs(lax.rem(i // wide_x, wide_y) - my_y)
            fx = jnp.abs(lax.rem(i, wide_x) - my_x)
            slot = (fy * 2 + fx) * wide_z + oz
            down_all[main:, pl.ds(pl.multiple_of(slot * down_cols, down_cols), down_cols)] = ext_all[i, 2]
            return 0

        lax.fori_loop(0, n_sp, lay, 0)

    wide_k = wide_z * down_cols
    wide_n = math.gcd(wide_k, 256)
    pieces = wide_k // wide_n

    def down_with(depth, k):
        def body(n, _):
            rows = group_rows(n // pieces)
            cols = pl.ds(pl.multiple_of(k * wide_k + lax.rem(n, pieces) * wide_n, wide_n), wide_n)
            term[rows, cols] = jnp.dot(
                hidden[rows, :depth], down_all[:depth, cols], preferred_element_type=f32
            ).astype(bf16)
            return 0

        lax.fori_loop(0, 2 * pieces, body, 0)

    sums, sums_far = [], []
    at_core = core * 2 * share

    def pair_sums(k):
        cols = pl.ds(k * wide_k, wide_k)
        away = pl.ds(pl.multiple_of((1 - core) * 2 * share, share), 2 * share)
        sums.append(to_pair(4 + k, term.at[away, cols], inbox2.at[:, cols]))
        sums[k].start()

    def far_sums(k):
        cols = pl.ds(k * wide_k, wide_k)
        sums[k].wait_recv()
        theirs_at = pl.multiple_of((1 - side) * share, share)
        psum[:, cols] = (
            term[pl.ds(pl.multiple_of(at_core + theirs_at, share), share), cols].astype(f32)
            + inbox2[pl.ds(theirs_at, share), cols].astype(f32)
        ).astype(bf16)
        sums_far.append(to_partner(8 + k, psum.at[:, cols], inbox3.at[:, cols]))
        sums_far[k].start()

    groups = ((0, 0), (0, 1), (1, 0), (1, 1))
    for k, (fy, fx) in enumerate(groups):
        if k:
            down_group(fy, fx)
        run(has_extra, lambda k=k: down_with(main + extra, k))
        run(jnp.logical_not(has_extra), lambda k=k: down_with(main, k))
        pair_sums(k)
        far_sums(k)

    def drain(ref, sem):
        pltpu.make_async_copy(ref, ref, sem).wait()

    for z in range(wide_z):
        @pl.when(my_z == z)
        def _(z=z):
            up = 1 if z + 1 < wide_z else 0
            drain(lat_all.at[pl.ds(0, (up + 3) * (z + 1) * half)], lat_send.at[0])
            drain(lat_all.at[pl.ds(0, (layer * (z + 1) - 1) * half)], lat_send.at[1])
            two = (1 if z + 2 < wide_z else 0) + (1 if z >= 2 else 0)
            one = up + (1 if z >= 1 else 0)
            on = (z if z + 2 < wide_z else 0) + (wide_z - 1 - z if z >= 2 else 0)
            n = two + one + on + 3 * wide_z
            drain(gate_all.at[pl.ds(0, n * gate_rows)], send.at[0])
            drain(up_all.at[pl.ds(0, n * gate_rows)], send.at[1])
            drain(down_all.at[pl.ds(0, main), pl.ds(0, n * down_cols)], send.at[2])
            run(has_extra, lambda: drain(ext_all.at[pl.ds(0, two + on + 3 * wide_z)], send.at[3]))
            run(jnp.logical_not(has_extra), lambda: drain(ext_all.at[pl.ds(0, one)], send.at[3]))

    for copy in [rows_out, rows_far, rows_on] + sums:
        copy.wait_send()

    mine_at = pl.multiple_of(side * share, share)
    for k, (fy, fx) in enumerate(groups):
        sums_far[k].wait_recv()

        def finish(t, _, k=k, fy=fy, fx=fx):
            slot = pl.ds(pl.multiple_of((k * wide_z + t) * down_cols, down_cols), down_cols)
            i = (t * wide_y + my_y + fy * (1 - 2 * my_y)) * wide_x + my_x + fx * (1 - 2 * my_x)
            cols = pl.ds(pl.multiple_of(i * down_cols, down_cols), down_cols)
            summed = (
                term[pl.ds(pl.multiple_of(at_core + mine_at, share), share), slot].astype(f32)
                + inbox2[pl.ds(mine_at, share), slot].astype(f32)
                + inbox3[:, slot].astype(f32)
            )
            out[:, cols] = (kept[:, cols].astype(f32) + 0.5 * summed).astype(bf16)
            return 0

        lax.fori_loop(0, wide_z, finish, 0)
    for copy in sums_far:
        copy.wait_send()


def fused_shards(
    grid, residual_in, query_lean, query_broad, latent, rope_key, latent_gain, key_up_lean,
    key_up_broad, value_up_lean, value_up_broad, out_lean, out_broad, attn_gain, mlp_gain,
    gate_weight, up_weight, down_weight,
):
    bf16, f32 = jnp.bfloat16, jnp.float32
    tokens = query_lean.shape[0]
    share, features = residual_in.shape
    rank = latent.shape[1]
    rope = rope_key.shape[1]
    n_sp = lax.axis_size("sp")
    positions = lax.axis_index("sp") * tokens + jnp.arange(tokens, dtype=jnp.int32)

    ql, qb = (jnp.transpose(query, (1, 2, 0)) for query in (query_lean, query_broad))
    freqs = THETA ** (-2.0 * jnp.arange(rope // 2, dtype=f32) / rope)
    angle = freqs[:, None] * positions.astype(f32)[None, :]
    lat = normalize(latent.astype(f32), latent_gain).astype(bf16)
    rot_key = rotate(rope_key.astype(f32), positions).astype(bf16)
    lat = jnp.concatenate([lat, rot_key.T], axis=0)
    kul = key_up_lean.reshape(rank, -1).T
    kub = key_up_broad.reshape(rank, -1).T
    vul = value_up_lean.reshape(rank, -1).T
    vub = value_up_broad.reshape(rank, -1).T
    wol = out_lean.reshape(-1, features)
    wob = out_broad.reshape(-1, features)
    heads = ql.shape[0] + qb.shape[0]
    units = gate_weight.shape[1]
    extra = gate_weight.shape[0]
    main = (units - extra) // 2
    wide_b = value_up_broad.shape[2]
    vmem = pl.BlockSpec(memory_space=pltpu.VMEM)
    args = (
        residual_in, ql, qb, lat, jnp.cos(angle), jnp.sin(angle), attn_gain[None], mlp_gain[None],
        kul, kub, vul, vub, wol, wob,
        gate_weight, up_weight, down_weight,
    )
    dma = pltpu.SemaphoreType.DMA
    return pl.pallas_call(
        functools.partial(layer_kernel, grid, (tokens, share, rope)),
        out_shape=jax.ShapeDtypeStruct((share, features), bf16),
        in_specs=[
            pl.BlockSpec(memory_space=pl.ANY) if k in (0, 12, 13, 14, 15, 16) else vmem for k in range(len(args))
        ],
        out_specs=vmem,
        scratch_shapes=[
            pltpu.VMEM((n_sp * (tokens + rope), rank), bf16),
            pltpu.VMEM((features, main), bf16),
            pltpu.VMEM((features, main), bf16),
            pltpu.VMEM((main + extra, features), bf16),
            pltpu.VMEM((n_sp, 3, extra, extra), bf16),
            pltpu.VMEM(gate_weight.shape, bf16),
            pltpu.VMEM(up_weight.shape, bf16),
            pltpu.VMEM(down_weight.shape, bf16),
            pltpu.VMEM((3, extra, extra), bf16),
            pltpu.VMEM(ql.shape, bf16),
            pltpu.VMEM(qb.shape, bf16),
            pltpu.VMEM(ql.shape, bf16),
            pltpu.VMEM(qb.shape, bf16),
            pltpu.VMEM((vul.shape[0], tokens), bf16),
            pltpu.VMEM((vub.shape[0], tokens), bf16),
            pltpu.VMEM((heads, 1, tokens), f32),
            pltpu.VMEM((heads, 1, tokens), f32),
            pltpu.VMEM((ql.shape[0], value_up_lean.shape[2], tokens), f32),
            pltpu.VMEM((qb.shape[0], wide_b, tokens), f32),
            pltpu.VMEM((tokens, vul.shape[0] + vub.shape[0]), bf16),
            pltpu.VMEM((2 * tokens, features), bf16),
            pltpu.VMEM((share, features), bf16),
            pltpu.VMEM((share, features), bf16),
            pltpu.VMEM((2 * tokens, features), bf16),
            pltpu.VMEM((2 * tokens, main + extra), bf16),
            pltpu.VMEM((2 * share, features), bf16),
            pltpu.VMEM((share, features), bf16),
            pltpu.VMEM((share, features), bf16),
            pltpu.VMEM(wol.shape, bf16),
            pltpu.VMEM(wob.shape, bf16),
            pltpu.VMEM(residual_in.shape, bf16),
            dma((n_sp,)),
            dma((2,)),
            dma((n_sp,)),
            dma((4, n_sp)),
            dma((4,)),
            dma((10,)),
            dma((12,)),
            dma((12,)),
        ],
        compiler_params=pltpu.CompilerParams(
            collective_id=0, has_side_effects=True, vmem_limit_bytes=62 * 2**20
        ),
    )(*args)


def fits(grid, mesh, args):
    if grid is None or mesh.shape["tp"] != 2 or grid[1] != 2 or grid[2] != 2 or grid[0] not in (2, 4, 6, 8):
        return False
    n_sp = mesh.shape["sp"]
    tokens = args[1].shape[0] // n_sp
    share = tokens // 2
    units = args[14].shape[1] // 2
    heads_l, heads_b = args[6].shape[1] // 2, args[7].shape[1] // 2
    wide_l, wide_b = args[6].shape[2], args[7].shape[2]
    rope = args[4].shape[1]
    return (
        tokens % 128 == 0 and tokens <= 256 and share % 16 == 0 and units >= 384
        and units % 256 == 128 and heads_l % 2 == 0 and 2 * wide_l == wide_b and wide_b % 128 == 0
        and args[3].shape[1] == tokens and rope % 32 == 0 and (tokens + rope) % 32 == 0
        and heads_b > 0 and args[8].shape[2] == wide_l and args[9].shape[2] == wide_b
        and args[14].shape[0] // n_sp == 128 and args[16].shape[1] // n_sp == 128
    )


def solution(mesh):
    in_specs = (
        P(("sp", "tp"), None),
        P("sp", "tp", None),
        P("sp", "tp", None),
        P("sp", None),
        P("sp", None),
        P(),
        P(None, "tp", None),
        P(None, "tp", None),
        P(None, "tp", None),
        P(None, "tp", None),
        P("tp", None, None),
        P("tp", None, None),
        P(),
        P(),
        P("sp", "tp"),
        P("sp", "tp"),
        P("tp", "sp"),
    )
    out_specs = P(("sp", "tp"), None)
    grid = grid_of(mesh)

    def layer(*args):
        body = functools.partial(fused_shards, grid) if fits(grid, mesh, args) else shards
        return jax.shard_map(
            body, mesh=mesh, in_specs=in_specs, out_specs=out_specs, check_vma=False
        )(*args)

    return layer
```

```python
import functools
import math

import jax
import jax.numpy as jnp
from jax import lax
from jax.experimental import pallas as pl
from jax.experimental.pallas import tpu as pltpu
from jax.sharding import PartitionSpec as P

THETA = 10000.0
EPS = 1e-06
NEGATIVE = -1e30


def rotate(values, positions):
    width = values.shape[-1]
    half = width // 2
    freqs = THETA ** (-2.0 * jnp.arange(half, dtype=jnp.float32) / width)
    angle = positions.astype(jnp.float32)[:, None] * freqs[None, :]
    cosine = jnp.cos(angle)
    sine = jnp.sin(angle)
    if values.ndim == 3:
        cosine = cosine[:, None, :]
        sine = sine[:, None, :]
    first = values[..., :half]
    second = values[..., half:]
    return jnp.concatenate(
        [first * cosine - second * sine, first * sine + second * cosine], axis=-1
    )


def normalize(values, gain):
    return values * lax.rsqrt(jnp.mean(values * values, axis=-1, keepdims=True) + EPS) * gain


def block_keys(weights, latent_rows):
    projected = []
    for key_up, value_up in weights:
        keys = jnp.einsum(
            "kr,rhd->khd", latent_rows, key_up, preferred_element_type=jnp.float32
        ).astype(jnp.bfloat16)
        values = jnp.einsum(
            "kr,rhd->khd", latent_rows, value_up, preferred_element_type=jnp.float32
        ).astype(jnp.bfloat16)
        projected.append((keys, values))
    return projected


def attend(carry, queries, projected, rotated_rows, key_pos, query_pos):
    updated = []
    visible = key_pos[None, :] <= query_pos[:, None]
    for state, query, pair in zip(carry, queries, projected):
        query_nope, query_rot, scale = query
        keys, values = pair
        peak, total, accum = state
        scores = (
            jnp.einsum("qhd,khd->hqk", query_nope, keys, preferred_element_type=jnp.float32)
            + jnp.einsum("qhr,kr->hqk", query_rot, rotated_rows, preferred_element_type=jnp.float32)
        ) * scale
        scores = jnp.where(visible[None], scores, NEGATIVE)
        new_peak = jnp.maximum(peak, jnp.max(scores, axis=-1))
        weights = jnp.where(visible[None], jnp.exp(scores - new_peak[..., None]), 0.0)
        factor = jnp.exp(peak - new_peak)
        total = total * factor + jnp.sum(weights, axis=-1)
        accum = accum * factor[..., None] + jnp.einsum(
            "hqk,khv->hqv", weights.astype(jnp.bfloat16), values, preferred_element_type=jnp.float32
        )
        updated.append((new_peak, total, accum))
    return tuple(updated)


def fold_piece(carry, latent_piece, rotated_piece, piece_pos, weights, segments):
    count = latent_piece.shape[0]
    block = math.gcd(count, 1024)
    last_all = segments[0][1][-1]

    def one_block(index, state):
        lat_rows = lax.dynamic_slice_in_dim(latent_piece, index * block, block, 0)
        rot_rows = lax.dynamic_slice_in_dim(rotated_piece, index * block, block, 0)
        pos_rows = lax.dynamic_slice_in_dim(piece_pos, index * block, block, 0)
        first_key = jnp.min(pos_rows)

        def work(inner):
            projected = block_keys(weights, lat_rows)
            results = []
            for inner_seg, segment in zip(inner, segments):
                queries, seg_pos = segment
                results.append(
                    lax.cond(
                        first_key <= seg_pos[-1],
                        lambda held, queries=queries, seg_pos=seg_pos: attend(
                            held, queries, projected, rot_rows, pos_rows, seg_pos
                        ),
                        lambda held: held,
                        inner_seg,
                    )
                )
            return tuple(results)

        return lax.cond(first_key <= last_all, work, lambda inner: inner, state)

    return lax.fori_loop(0, count // block, one_block, carry)


def shards(
    residual_in,
    query_lean,
    query_broad,
    latent,
    rope_key,
    latent_gain,
    key_up_lean,
    key_up_broad,
    value_up_lean,
    value_up_broad,
    out_lean,
    out_broad,
    attn_gain,
    mlp_gain,
    gate_weight,
    up_weight,
    down_weight,
):
    tokens_here = query_lean.shape[0]
    n_tp = lax.axis_size("tp")
    share = tokens_here // n_tp
    sp_index = lax.axis_index("sp")
    first = sp_index * tokens_here
    query_pos = first + jnp.arange(tokens_here, dtype=jnp.int32)
    rope_width = rope_key.shape[1]
    weights = ((key_up_lean, value_up_lean), (key_up_broad, value_up_broad))
    segment_rows = (query_lean, query_broad, query_pos)
    segments = []
    initial = []
    lean_rows, broad_rows, seg_pos = segment_rows
    queries = []
    states = []
    for query, value_up in ((lean_rows, value_up_lean), (broad_rows, value_up_broad)):
        nope = query.shape[2] - rope_width
        query_rot = rotate(query[:, :, nope:].astype(jnp.float32), seg_pos).astype(jnp.bfloat16)
        queries.append((query[:, :, :nope], query_rot, query.shape[2] ** (-0.5)))
        heads = query.shape[1]
        rows = query.shape[0]
        states.append(
            (
                jnp.full((heads, rows), NEGATIVE, jnp.float32),
                jnp.zeros((heads, rows), jnp.float32),
                jnp.zeros((heads, rows, value_up.shape[2]), jnp.float32),
            )
        )
    segments.append((tuple(queries), seg_pos))
    initial.append(tuple(states))
    segments = tuple(segments)
    initial = tuple(initial)
    sent_latent = normalize(latent.astype(jnp.float32), latent_gain).astype(jnp.bfloat16)
    sent_rot = rotate(rope_key.astype(jnp.float32), query_pos).astype(jnp.bfloat16)
    pieces = (
        lax.all_gather(sent_latent, "sp", axis=0, tiled=True),
        lax.all_gather(sent_rot, "sp", axis=0, tiled=True),
    )
    piece_pos = jnp.arange(pieces[0].shape[0], dtype=jnp.int32)
    folded = fold_piece(initial, pieces[0], pieces[1], piece_pos, weights, segments)
    results = [
        [(accum / total[..., None]).astype(jnp.bfloat16) for peak, total, accum in seg_state]
        for seg_state in folded
    ]
    attended = results[0]
    term = jnp.zeros((share * lax.axis_size("tp"), out_lean.shape[2]), jnp.float32)
    for rows_all, weight in ((attended[0], out_lean), (attended[1], out_broad)):
        rows = rows_all
        term = term + jnp.einsum("hqv,hvd->qd", rows, weight, preferred_element_type=jnp.float32)
    head_sum = lax.psum_scatter(
        term.astype(jnp.bfloat16), "tp", scatter_dimension=0, tiled=True
    ).astype(jnp.float32)
    branch = normalize(head_sum, attn_gain)
    kept = (residual_in.astype(jnp.float32) + branch).astype(jnp.bfloat16)
    normed = normalize(kept.astype(jnp.float32), mlp_gain).astype(jnp.bfloat16)
    whole_normed = lax.all_gather(normed, "tp", axis=0, tiled=True)
    gate_whole, up_whole, down_whole = (
        lax.all_gather(gate_weight, "sp", axis=0, tiled=True),
        lax.all_gather(up_weight, "sp", axis=0, tiled=True),
        lax.all_gather(down_weight, "sp", axis=1, tiled=True),
    )
    gate = jnp.dot(whole_normed, gate_whole, preferred_element_type=jnp.float32)
    up = jnp.dot(whole_normed, up_whole, preferred_element_type=jnp.float32)
    hidden = (jax.nn.silu(gate) * up).astype(jnp.bfloat16)
    rows = hidden
    channel_sum = lax.psum_scatter(
        jnp.dot(rows, down_whole, preferred_element_type=jnp.float32).astype(jnp.bfloat16),
        "tp",
        scatter_dimension=0,
        tiled=True,
    ).astype(jnp.float32)
    return (kept.astype(jnp.float32) + 0.5 * channel_sum).astype(jnp.bfloat16)


LOG2E = math.log2(math.e)


def grid_of(mesh):
    n_sp, n_tp = mesh.shape["sp"], mesh.shape["tp"]
    devices = mesh.devices.reshape(n_sp, n_tp)
    try:
        places = [tuple(device.coords) for device in devices[:, 0]]
        partners = [tuple(device.coords) for device in devices[:, -1]]
    except Exception:
        return (n_sp // 4, 2, 2) if n_sp % 4 == 0 else None
    if places != partners:
        return None
    low = [min(place[k] for place in places) for k in range(3)]
    sizes = [max(place[k] for place in places) - low[k] + 1 for k in range(3)]
    wide_z, wide_y, wide_x = sizes[2], sizes[1], sizes[0]
    if wide_z * wide_y * wide_x != n_sp:
        return None
    for index, place in enumerate(places):
        x, y, z = (place[k] - low[k] for k in range(3))
        if (z * wide_y + y) * wide_x + x != index:
            return None
    return wide_z, wide_y, wide_x


def hop_table(grid):
    wide_z = grid[0]
    entries = [
        (dz, fy, fx)
        for dz in range(1 - wide_z, wide_z)
        for fy in range(2)
        for fx in range(2)
        if (dz, fy, fx) != (0, 0, 0)
    ]
    entries.sort(key=lambda e: (abs(e[0]) + e[1] + e[2], abs(e[0]), e))
    return entries


def layer_kernel(
    grid, shapes, res_in, qlt, qbt, lat_in, rope_in, lg, ag, mg, kul, kub_in, vul, vub_in, wol_in, wob_in, gw, uw, dw, out,
    lat, kub, vub, cosine, sine, lat_all, gate_all, up_all, down_all, ext_all, own_g, own_u, own_d, own_e, ql, qb, keyn, scores, weigh, valt_l, valt_b,
    peak, total, acc_l, acc_b, att, term, inbox, kept, rows_all, hidden, inbox2, psum, inbox3, wol, wob, res,
    lat_recv, lat_send, lat_pair, recv, send, own_sem, pair_send, pair_recv,
):
    wide_z, wide_y, wide_x = grid
    n_sp = wide_z * wide_y * wide_x
    tokens, share, rope = shapes
    heads_l, heads_b = qlt.shape[0], qbt.shape[0]
    bf16, f32 = jnp.bfloat16, jnp.float32
    me = lax.axis_index("sp")
    core = lax.axis_index("tp")
    my_x = lax.rem(me, wide_x)
    my_y = lax.rem(me // wide_x, wide_y)
    my_z = me // (wide_x * wide_y)
    layer = wide_y * wide_x
    flip_y = me + (1 - 2 * my_y) * wide_x
    flip_x = me + (1 - 2 * my_x)
    side = lax.rem(my_z, 2)
    partner = me + (1 - 2 * side) * layer
    z_ways = [
        (step, my_z + step < wide_z if step > 0 else my_z + step >= 0,
         jnp.clip(me + step * layer, 0, n_sp - 1))
        for step in (1, -1, 2, -2)
    ]

    def z_way(step):
        return next(way for way in z_ways if way[0] == step)

    def run(condition, action):
        pl.when(condition)(action)

    gate_rows, units = gw.shape
    down_cols = dw.shape[1]
    extra = ext_all.shape[2]
    main = (units - extra) // 2
    fetch = [
        pltpu.make_async_copy(src, dst, own_sem.at[k])
        for k, (src, dst) in enumerate((
            (gw, own_g), (uw, own_u), (dw, own_d),
            (gw.at[:, pl.ds(2 * main, extra)], own_e.at[0]),
            (uw.at[:, pl.ds(2 * main, extra)], own_e.at[1]),
            (dw.at[pl.ds(2 * main, extra), :], own_e.at[2]),
            (wol_in, wol), (wob_in, wob), (res_in, res),
        ))
    ]
    for copy in fetch:
        copy.start()
    half_rope = rope // 2
    lane = lax.broadcasted_iota(jnp.int32, (half_rope, tokens), 1)
    line = lax.broadcasted_iota(jnp.int32, (half_rope, tokens), 0)
    freqs = jnp.zeros((half_rope, tokens), f32)
    for k in range(half_rope):
        freqs = jnp.where(line == k, THETA ** (-2.0 * k / rope), freqs)
    angle = (me * tokens + lane).astype(f32) * freqs
    cosine[...] = jnp.cos(angle)
    sine[...] = jnp.sin(angle)
    lat[:tokens, :] = normalize(lat_in[...].astype(f32), lg[...]).astype(bf16)
    one, two = rope_in[:half_rope, :].astype(f32), rope_in[half_rope:, :].astype(f32)
    lat[tokens:tokens + half_rope, :] = (one * cosine[...] - two * sine[...]).astype(bf16)
    lat[tokens + half_rope:, :] = (one * sine[...] + two * cosine[...]).astype(bf16)
    lat_rows = lat.shape[0]
    barrier = pltpu.get_barrier_semaphore()
    for where in (flip_x, flip_y):
        pl.semaphore_signal(barrier, inc=1, device_id={"sp": where})
    pl.semaphore_signal(barrier, inc=1, device_id={"tp": 1 - core})
    greeted = 3
    for _, exists, where in z_ways:
        run(exists, lambda where=where: pl.semaphore_signal(barrier, inc=1, device_id={"sp": where}))
        greeted = greeted + jnp.where(exists, 1, 0)
    pl.semaphore_wait(barrier, greeted)

    half = lat_rows // 2
    first = pl.multiple_of(core * half, 16)

    def lat_at(i):
        return lat_all.at[pl.ds(pl.multiple_of(i * lat_rows + first, 16), half)]

    def lat_copy(i, mine, where):
        return pltpu.make_async_remote_copy(
            src_ref=lat.at[pl.ds(first, half)] if mine else lat_at(i), dst_ref=lat_at(i),
            send_sem=lat_send.at[0], recv_sem=lat_recv.at[i], device_id={"sp": where},
        )

    def pair_lat(i):
        return pltpu.make_async_remote_copy(
            src_ref=lat_at(i), dst_ref=lat_at(i), send_sem=lat_send.at[1],
            recv_sem=lat_pair.at[i], device_id={"tp": 1 - core},
        )

    def lat_up(i, mine):
        _, exists, where = z_way(1)
        run(exists, lambda: lat_copy(i, mine, where).start())

    turn = jnp.where(core == 0, flip_x, flip_y)
    away = jnp.where(core == 0, flip_y, flip_x)
    lat_copy(me, True, turn).start()
    lat_copy(me, True, away).start()
    lat_up(me, True)

    per = 4

    def words_of(table):
        codes = [((dz + wide_z - 1) * 2 + fy) * 2 + fx for dz, fy, fx in table]
        return [
            sum(code << (7 * k) for k, code in enumerate(codes[at:at + per]))
            for at in range(0, len(codes), per)
        ]

    def origin_of(n, words):
        word = jnp.int32(words[0])
        for k in range(1, len(words)):
            word = jnp.where(n // per == k, jnp.int32(words[k]), word)
        rem = lax.rem(n, per)
        for k in range(1, per):
            word = jnp.where(rem >= k, word // 128, word)
        code = lax.rem(word, 128)
        return code // 4 - (wide_z - 1), lax.rem(code // 2, 2), lax.rem(code, 2)

    def index_of(dz, fy, fx):
        oy = my_y + fy * (1 - 2 * my_y)
        ox = my_x + fx * (1 - 2 * my_x)
        return ((my_z + dz) * wide_y + oy) * wide_x + ox

    def lat_event(i, on):
        lat_copy(i, False, turn).wait_recv()
        if on:
            lat_copy(i, False, away).start()
        lat_up(i, False)
        pair_lat(i).start()

    def lat_layer(down):
        @pl.when(my_z >= down)
        def _():
            def body(t, _):
                lat_event(index_of(-down, t // 2, lax.rem(t, 2)), False)
                return 0

            lax.fori_loop(0, layer, body, 0)

    lat_event(turn, True)
    lat_event(away, False)
    lat_event(index_of(0, 1, 1), False)

    def slot_at(ref, i):
        return ref.at[pl.ds(pl.multiple_of(i * gate_rows, gate_rows), gate_rows), pl.ds(0, main)]

    def down_slot(dz, fy, fx):
        slot = (fy * 2 + fx) * wide_z + my_z + dz
        return down_all.at[pl.ds(0, main), pl.ds(pl.multiple_of(slot * down_cols, down_cols), down_cols)]

    def place(p, dz, fy, fx):
        i = index_of(dz, fy, fx)
        if p == 0:
            return slot_at(gate_all, i)
        if p == 1:
            return slot_at(up_all, i)
        if p == 2:
            return down_slot(dz, fy, fx)
        return ext_all.at[i]

    def own_half(p, h):
        lanes = pl.ds(pl.multiple_of(h * main, extra), main)
        if p == 0:
            return own_g.at[:, lanes]
        if p == 1:
            return own_u.at[:, lanes]
        if p == 2:
            return own_d.at[lanes, :]
        return own_e

    def part_copy(p, src, dst, i, where):
        return pltpu.make_async_remote_copy(
            src_ref=src, dst_ref=dst, send_sem=send.at[p], recv_sem=recv.at[p, i], device_id={"sp": where},
        )

    has_extra = core == side

    def to_z(p, src, step, origin, i, condition=True):
        _, exists, where = z_way(step)
        dst = place(p, *origin) if p == 2 else place(p, *origin)
        run(jnp.logical_and(exists, condition), lambda: part_copy(p, src, dst, i, where).start())

    def seen(origin, fy, fx):
        return origin[0], origin[1] + fy - 2 * origin[1] * fy, origin[2] + fx - 2 * origin[2] * fx

    def dst_for(p, origin, fy, fx):
        if p == 2:
            return down_slot(*seen(origin, fy, fx))
        return place(p, *origin)

    def send_own(p, steps, in_layer, when=True):
        here = (0, 0, 0)
        mine = own_half(p, side)
        other = own_half(p, 1 - side)
        same = has_extra if p == 3 else True
        cross = jnp.logical_not(has_extra) if p == 3 else True
        for step in steps:
            if step in (1, -1):
                to_z(p, other, step, here, me, jnp.logical_and(cross, when))
            else:
                to_z(p, mine, step, here, me, jnp.logical_and(same, when))

        def flips():
            part_copy(p, mine, dst_for(p, here, 0, 1), me, flip_x).start()
            part_copy(p, mine, dst_for(p, here, 1, 0), me, flip_y).start()

        if in_layer and p == 3:
            run(has_extra, flips)
        elif in_layer:
            flips()

    def part_event(p, dz, fy, fx):
        origin = (dz, fy, fx)
        i = index_of(*origin)
        here = place(p, *origin)
        part_copy(p, here, here, i, flip_x).wait_recv()
        column = jnp.logical_and(fy == 0, fx == 0)
        to_z(p, here, 2, origin, i, jnp.logical_and(column, dz < 0))
        to_z(p, here, -2, origin, i, jnp.logical_and(column, dz > 0))
        x_line = jnp.logical_and(fy == 0, fx == 1)
        y_line = jnp.logical_and(fy == 1, fx == 0)
        if p == 0:
            to_x, to_y = column, jnp.logical_or(column, x_line)
        elif p == 1:
            to_x, to_y = jnp.logical_or(column, y_line), column
        else:
            x_first = core == 0 if p == 2 else lax.rem(my_z + dz, 2) == 0
            to_x = jnp.logical_or(column, jnp.logical_and(y_line, jnp.logical_not(x_first)))
            to_y = jnp.logical_or(column, jnp.logical_and(x_line, x_first))
        run(to_x, lambda: part_copy(p, here, dst_for(p, origin, 0, 1), i, flip_x).start())
        run(to_y, lambda: part_copy(p, here, dst_for(p, origin, 1, 0), i, flip_y).start())

    for copy in fetch[:6]:
        copy.wait()
    everything = (0, 1, 3, 2)
    for p in everything:
        send_own(p, (-1, -2), True)
    lat_layer(1)
    for p in everything:
        send_own(p, (1, 2), False, my_z <= 1)

    whole = hop_table(grid)
    whole_words = words_of(whole)
    count = len(whole)
    hops = [abs(dz) + fy + fx for dz, fy, fx in whole]
    early = sum(1 for hop in hops if hop <= 2)
    lag = sum(1 for hop in hops if hop >= wide_z)

    def events(low, high):
        def gates(n):
            dz, fy, fx = origin_of(n, whole_words)

            @pl.when(jnp.logical_and(my_z + dz >= 0, my_z + dz < wide_z))
            def _():
                part_event(0, dz, fy, fx)
                part_event(1, dz, fy, fx)
                run(has_extra, lambda: part_event(3, dz, fy, fx))

        def downs(n):
            dz, fy, fx = origin_of(n, whole_words)
            run(
                jnp.logical_and(my_z + dz >= 0, my_z + dz < wide_z),
                lambda: part_event(2, dz, fy, fx),
            )

        def body(t, _):
            run(t < count, lambda: gates(t))
            run(t >= lag, lambda: downs(t - lag))
            return 0

        lax.fori_loop(low, high, body, 0)

    own_rows = pl.ds(pl.multiple_of(me * gate_rows, gate_rows), gate_rows)
    own_lanes = pl.ds(pl.multiple_of(side * main, extra), main)
    gate_all[own_rows, :main] = own_g[:, own_lanes]
    up_all[own_rows, :main] = own_u[:, own_lanes]
    down_all[:main, pl.ds(pl.multiple_of(my_z * down_cols, down_cols), down_cols)] = own_d[own_lanes, :]
    ext_all[me] = own_e[...]

    wide_l = kul.shape[0] // heads_l
    wide_b = kub.shape[1] // heads_b
    for h in range(heads_b):
        part = slice(h * wide_b, (h + 1) * wide_b)
        kub[:, part] = kub_in[:, h, :]
        vub[part, :] = vub_in[:, h, :].T
    for given, query in ((qlt, ql), (qbt, qb)):
        nope = given.shape[1] - rope
        for h in range(given.shape[0]):
            one = given[h, nope:nope + half_rope, :].astype(f32)
            two = given[h, nope + half_rope:, :].astype(f32)
            if nope < wide_b:
                query[h, :wide_b, :] = jnp.zeros((wide_b, tokens), bf16)
            at = (h * nope) % wide_b
            query[h, at:at + nope, :] = given[h, :nope, :]
            query[h, wide_b:wide_b + half_rope, :] = (one * cosine[...] - two * sine[...]).astype(bf16)
            query[h, wide_b + half_rope:, :] = (one * sine[...] + two * cosine[...]).astype(bf16)
    lat_all[pl.ds(pl.multiple_of(me * lat_rows, 16), lat_rows), :] = lat[...]

    peak[...] = jnp.full(peak.shape, NEGATIVE, f32)
    total[...] = jnp.zeros(total.shape, f32)
    acc_l[...] = jnp.zeros(acc_l.shape, f32)
    acc_b[...] = jnp.zeros(acc_b.shape, f32)
    contract = (((1,), (1,)), ((), ()))
    strip = math.gcd(tokens, 64)
    strips = [slice(at, at + strip) for at in range(0, tokens, strip)]

    def attend_block(j, masked):
        at_j = pl.multiple_of(j * lat_rows, 16)
        rows = lat_all[pl.ds(at_j, tokens), :]
        rot = lat_all[pl.ds(pl.multiple_of(at_j + tokens, 16), rope), :].T
        split = heads_l * wide_l
        keyn[:, :split] = lax.dot_general(rows, kul[...], contract, preferred_element_type=f32).astype(bf16)
        keyn[:, split:] = jnp.dot(rows, kub[...], preferred_element_type=f32).astype(bf16)
        for ups, held in ((vul, valt_l), (vub, valt_b)):
            held[...] = lax.dot_general(
                ups[...], rows, contract, preferred_element_type=f32
            ).astype(bf16)

        def of(g):
            if g < heads_l:
                return g, ql, valt_l, acc_l, wide_l, wide_l + rope
            return g - heads_l, qb, valt_b, acc_b, wide_b, wide_b + rope

        def score(g):
            h, query = of(g)[:2]
            at = (g * wide_l // wide_b if g < heads_l else split // wide_b + h) * wide_b
            keys = jnp.concatenate([keyn[:, at:at + wide_b], rot], axis=1)
            held = jnp.dot(keys, query[h], preferred_element_type=f32)
            if masked:
                key_pos = lax.broadcasted_iota(jnp.int32, (tokens, tokens), 0)
                visible = key_pos <= lax.broadcasted_iota(jnp.int32, (tokens, tokens), 1)
                held = jnp.where(visible, held, NEGATIVE)
            scores[g % 2] = held

        score(0)
        for g in range(heads_l + heads_b):
            if g + 1 < heads_l + heads_b:
                score(g + 1)
            h, query, held, acc, wide, size = of(g)
            scale = LOG2E * size ** (-0.5)
            old = peak[g]
            top = jnp.max(scores[g % 2, strips[0], :], axis=0, keepdims=True)
            for part in strips[1:]:
                top = jnp.maximum(top, jnp.max(scores[g % 2, part, :], axis=0, keepdims=True))
            new = jnp.maximum(old, top * scale)
            factor = jnp.exp2(old - new)
            summed = total[g] * factor
            for part in strips:
                weights = jnp.exp2(scores[g % 2, part, :] * scale - new)
                summed = summed + jnp.sum(weights, axis=0, keepdims=True)
                weigh[g % 2, part, :] = weights.astype(bf16)
            peak[g] = new
            total[g] = summed
            acc[h] = acc[h] * factor + jnp.dot(
                held[h * wide:(h + 1) * wide, :], weigh[g % 2], preferred_element_type=f32
            )

    def attend_layer(down, low, high):
        def body(t, _):
            events(low + (t * (high - low)) // layer, low + ((t + 1) * (high - low)) // layer)
            i = (my_z - down) * layer + t

            @pl.when(jnp.logical_and(my_z >= down, i < me))
            def _():
                pair_lat(i).wait_recv()
                attend_block(i, False)

            return 0

        lax.fori_loop(0, layer, body, 0)

    attend_block(me, True)
    attend_layer(0, 0, 0)
    for down in range(1, wide_z):
        if down + 1 < wide_z:
            lat_layer(down + 1)
            for p in everything:
                send_own(p, (1, 2), False, my_z == down + 1)
        attend_layer(down, (down - 1) * early // (wide_z - 1), down * early // (wide_z - 1))

    def rest(i, _):
        run(jnp.logical_and(i > me, i < (my_z + 1) * layer), lambda: pair_lat(i).wait_recv())
        return 0

    lax.fori_loop(0, n_sp, rest, 0)

    split = heads_l * wide_l
    for heads, wide, acc, base, col in (
        (heads_l, wide_l, acc_l, 0, 0), (heads_b, wide_b, acc_b, heads_l, split),
    ):
        together = wide_b // wide
        for h in range(0, heads, together):
            done = jnp.concatenate(
                [acc[h + k] / total[base + h + k] for k in range(together)], axis=0
            )
            att[:, col + h * wide:col + (h + together) * wide] = done.T.astype(bf16)

    features = out.shape[1]
    block = math.gcd(features, 512)

    for copy in fetch[6:]:
        copy.wait()

    def project(n, _):
        cols = pl.ds(pl.multiple_of(n * block, block), block)
        term[:tokens, cols] = (
            jnp.dot(att[:, :split], wol[:, cols], preferred_element_type=f32)
            + jnp.dot(att[:, split:], wob[:, cols], preferred_element_type=f32)
        ).astype(bf16)
        return 0

    lax.fori_loop(0, features // block, project, 0)
    theirs = pl.ds(pl.multiple_of((1 - core) * share, share), share)

    def to_pair(k, src, dst):
        return pltpu.make_async_remote_copy(
            src_ref=src, dst_ref=dst, send_sem=pair_send.at[k], recv_sem=pair_recv.at[k],
            device_id={"tp": 1 - core},
        )

    def to_partner(k, src, dst):
        return pltpu.make_async_remote_copy(
            src_ref=src, dst_ref=dst, send_sem=pair_send.at[k], recv_sem=pair_recv.at[k],
            device_id={"sp": partner},
        )

    def place_of(of_core, of_side):
        return pl.ds(pl.multiple_of((of_core * 2 + of_side) * share, share), share)

    heads_out = to_pair(0, term.at[theirs], inbox)
    heads_out.start()
    heads_out.wait_recv()
    rows_at_once = math.gcd(share, 16)

    def norms(n, _):
        rows = pl.ds(pl.multiple_of(n * rows_at_once, rows_at_once), rows_at_once)
        full = pl.ds(pl.multiple_of(core * share + n * rows_at_once, rows_at_once), rows_at_once)
        spot = pl.ds(pl.multiple_of((core * 2 + side) * share + n * rows_at_once, rows_at_once), rows_at_once)
        summed = term[full, :].astype(f32) + inbox[rows, :].astype(f32)
        branch = normalize(summed, ag[...])
        mixed = (res[rows, :].astype(f32) + branch).astype(bf16)
        kept[rows, :] = mixed
        rows_all[spot, :] = normalize(mixed.astype(f32), mg[...]).astype(bf16)
        return 0

    lax.fori_loop(0, share // rows_at_once, norms, 0)
    mine_at = rows_all.at[place_of(core, side)]
    rows_out = to_pair(1, mine_at, mine_at)
    rows_far = to_partner(2, mine_at, mine_at)
    rows_out.start()
    rows_far.start()
    heads_out.wait_send()
    ready = sum(1 for hop in hops if hop < wide_z)
    events(early, ready)
    far_at = rows_all.at[place_of(core, 1 - side)]
    to_partner(2, far_at, far_at).wait_recv()
    rows_on = to_pair(3, far_at, far_at)
    rows_on.start()
    near_at = rows_all.at[place_of(1 - core, side)]
    to_pair(1, near_at, near_at).wait_recv()
    last_at = rows_all.at[place_of(1 - core, 1 - side)]
    to_pair(3, last_at, last_at).wait_recv()
    events(ready, count)

    def feed_from(rows, gate_w, up_w, cols):
        gate = jnp.dot(rows_all[rows, :], gate_w, preferred_element_type=f32)
        up = jnp.dot(rows_all[rows, :], up_w, preferred_element_type=f32)
        hidden[rows, cols] = (gate / (1.0 + jnp.exp(-gate)) * up).astype(bf16)

    span = 256
    chunks = main // span
    group = tokens

    def group_rows(n):
        return pl.ds(pl.multiple_of(n * group, group), group)

    @pl.when(has_extra)
    def _():
        def lay(i, _):
            oz = i // layer
            fy = jnp.abs(lax.rem(i // wide_x, wide_y) - my_y)
            fx = jnp.abs(lax.rem(i, wide_x) - my_x)
            slot = (fy * 2 + fx) * wide_z + oz
            at_i = pl.ds(pl.multiple_of(i * gate_rows, gate_rows), gate_rows)
            gate_all[at_i, main:] = ext_all[i, 0]
            up_all[at_i, main:] = ext_all[i, 1]
            down_all[main:, pl.ds(pl.multiple_of(slot * down_cols, down_cols), down_cols)] = ext_all[i, 2]
            return 0

        lax.fori_loop(0, n_sp, lay, 0)

    def feed_loop(n, _):
        rows = group_rows(n // chunks)
        cols = pl.ds(pl.multiple_of(lax.rem(n, chunks) * span, span), span)
        feed_from(rows, gate_all[:, cols], up_all[:, cols], cols)
        return 0

    lax.fori_loop(0, 2 * chunks, feed_loop, 0)

    def feed_rest(high):
        def body(n, _):
            cols = slice(chunks * span, high)
            feed_from(group_rows(n), gate_all[:, cols], up_all[:, cols], cols)
            return 0

        if high > chunks * span:
            lax.fori_loop(0, 2, body, 0)

    run(has_extra, lambda: feed_rest(main + extra))
    run(jnp.logical_not(has_extra), lambda: feed_rest(main))

    wide_k = wide_z * down_cols
    wide_n = math.gcd(wide_k, 256)
    pieces = wide_k // wide_n

    def down_with(depth, k):
        def body(n, _):
            rows = group_rows(n // pieces)
            cols = pl.ds(pl.multiple_of(k * wide_k + lax.rem(n, pieces) * wide_n, wide_n), wide_n)
            term[rows, cols] = jnp.dot(
                hidden[rows, :depth], down_all[:depth, cols], preferred_element_type=f32
            ).astype(bf16)
            return 0

        lax.fori_loop(0, 2 * pieces, body, 0)

    sums, sums_far = [], []
    at_core = core * 2 * share

    def pair_sums(k):
        cols = pl.ds(k * wide_k, wide_k)
        away = pl.ds(pl.multiple_of((1 - core) * 2 * share, share), 2 * share)
        sums.append(to_pair(4 + k, term.at[away, cols], inbox2.at[:, cols]))
        sums[k].start()

    def far_sums(k):
        cols = pl.ds(k * wide_k, wide_k)
        sums[k].wait_recv()
        theirs_at = pl.multiple_of((1 - side) * share, share)
        psum[:, cols] = (
            term[pl.ds(pl.multiple_of(at_core + theirs_at, share), share), cols].astype(f32)
            + inbox2[pl.ds(theirs_at, share), cols].astype(f32)
        ).astype(bf16)
        sums_far.append(to_partner(8 + k, psum.at[:, cols], inbox3.at[:, cols]))
        sums_far[k].start()

    groups = ((0, 0), (0, 1), (1, 0), (1, 1))
    last = sum(1 for hop in hops if hop > wide_z)
    for k, (fy, fx) in enumerate(groups):
        if k == 1:
            events(count, count + lag - last)
        if k == 3:
            events(count + lag - last, count + lag)
        run(has_extra, lambda k=k: down_with(main + extra, k))
        run(jnp.logical_not(has_extra), lambda k=k: down_with(main, k))
        pair_sums(k)
        if k:
            far_sums(k - 1)
    far_sums(len(groups) - 1)

    def drain(ref, sem):
        pltpu.make_async_copy(ref, ref, sem).wait()

    for z in range(wide_z):
        @pl.when(my_z == z)
        def _(z=z):
            up = 1 if z + 1 < wide_z else 0
            drain(lat_all.at[pl.ds(0, (up * layer * (z + 1) + 3) * half)], lat_send.at[0])
            drain(lat_all.at[pl.ds(0, (layer * (z + 1) - 1) * half)], lat_send.at[1])
            two = (1 if z + 2 < wide_z else 0) + (1 if z >= 2 else 0)
            one = up + (1 if z >= 1 else 0)
            on = (z if z + 2 < wide_z else 0) + (wide_z - 1 - z if z >= 2 else 0)
            n = two + one + on + 3 * wide_z
            drain(gate_all.at[pl.ds(0, n * gate_rows), pl.ds(0, main)], send.at[0])
            drain(up_all.at[pl.ds(0, n * gate_rows), pl.ds(0, main)], send.at[1])
            drain(down_all.at[pl.ds(0, main), pl.ds(0, n * down_cols)], send.at[2])
            run(has_extra, lambda: drain(ext_all.at[pl.ds(0, two + on + 3 * wide_z)], send.at[3]))
            run(jnp.logical_not(has_extra), lambda: drain(ext_all.at[pl.ds(0, one)], send.at[3]))

    for copy in [rows_out, rows_far, rows_on] + sums:
        copy.wait_send()

    mine_at = pl.multiple_of(side * share, share)
    for k, (fy, fx) in enumerate(groups):
        sums_far[k].wait_recv()

        def finish(t, _, k=k, fy=fy, fx=fx):
            slot = pl.ds(pl.multiple_of((k * wide_z + t) * down_cols, down_cols), down_cols)
            i = (t * wide_y + my_y + fy * (1 - 2 * my_y)) * wide_x + my_x + fx * (1 - 2 * my_x)
            cols = pl.ds(pl.multiple_of(i * down_cols, down_cols), down_cols)
            summed = (
                term[pl.ds(pl.multiple_of(at_core + mine_at, share), share), slot].astype(f32)
                + inbox2[pl.ds(mine_at, share), slot].astype(f32)
                + inbox3[:, slot].astype(f32)
            )
            out[:, cols] = (kept[:, cols].astype(f32) + 0.5 * summed).astype(bf16)
            return 0

        lax.fori_loop(0, wide_z, finish, 0)
    for copy in sums_far:
        copy.wait_send()


def fused_shards(
    grid, residual_in, query_lean, query_broad, latent, rope_key, latent_gain, key_up_lean,
    key_up_broad, value_up_lean, value_up_broad, out_lean, out_broad, attn_gain, mlp_gain,
    gate_weight, up_weight, down_weight,
):
    bf16, f32 = jnp.bfloat16, jnp.float32
    tokens = query_lean.shape[0]
    share, features = residual_in.shape
    rank = latent.shape[1]
    rope = rope_key.shape[1]
    n_sp = lax.axis_size("sp")
    ql, qb = (jnp.transpose(query, (1, 2, 0)) for query in (query_lean, query_broad))
    kul = key_up_lean.reshape(rank, -1).T
    vul = value_up_lean.reshape(rank, -1).T
    wol = out_lean.reshape(-1, features)
    wob = out_broad.reshape(-1, features)
    heads = ql.shape[0] + qb.shape[0]
    wide_all = qb.shape[0] * value_up_broad.shape[2]
    units = gate_weight.shape[1]
    extra = gate_weight.shape[0]
    main = (units - extra) // 2
    wide_b = value_up_broad.shape[2]
    vmem = pl.BlockSpec(memory_space=pltpu.VMEM)
    args = (
        residual_in, ql, qb, latent, rope_key.T, latent_gain[None], attn_gain[None], mlp_gain[None],
        kul, key_up_broad, vul, value_up_broad, wol, wob,
        gate_weight, up_weight, down_weight,
    )
    dma = pltpu.SemaphoreType.DMA
    return pl.pallas_call(
        functools.partial(layer_kernel, grid, (tokens, share, rope)),
        out_shape=jax.ShapeDtypeStruct((share, features), bf16),
        in_specs=[
            pl.BlockSpec(memory_space=pl.ANY) if k in (0, 12, 13, 14, 15, 16) else vmem for k in range(len(args))
        ],
        out_specs=vmem,
        scratch_shapes=[
            pltpu.VMEM((tokens + rope, rank), bf16),
            pltpu.VMEM((rank, wide_all), bf16),
            pltpu.VMEM((wide_all, rank), bf16),
            pltpu.VMEM((rope // 2, tokens), f32),
            pltpu.VMEM((rope // 2, tokens), f32),
            pltpu.VMEM((n_sp * (tokens + rope), rank), bf16),
            pltpu.VMEM((features, main + extra), bf16),
            pltpu.VMEM((features, main + extra), bf16),
            pltpu.VMEM((main + extra, features), bf16),
            pltpu.VMEM((n_sp, 3, extra, extra), bf16),
            pltpu.VMEM(gate_weight.shape, bf16),
            pltpu.VMEM(up_weight.shape, bf16),
            pltpu.VMEM(down_weight.shape, bf16),
            pltpu.VMEM((3, extra, extra), bf16),
            pltpu.VMEM((ql.shape[0],) + qb.shape[1:], bf16),
            pltpu.VMEM(qb.shape, bf16),
            pltpu.VMEM((tokens, kul.shape[0] + wide_all), bf16),
            pltpu.VMEM((2, tokens, tokens), f32),
            pltpu.VMEM((2, tokens, tokens), bf16),
            pltpu.VMEM((vul.shape[0], tokens), bf16),
            pltpu.VMEM((wide_all, tokens), bf16),
            pltpu.VMEM((heads, 1, tokens), f32),
            pltpu.VMEM((heads, 1, tokens), f32),
            pltpu.VMEM((ql.shape[0], value_up_lean.shape[2], tokens), f32),
            pltpu.VMEM((qb.shape[0], wide_b, tokens), f32),
            pltpu.VMEM((tokens, vul.shape[0] + wide_all), bf16),
            pltpu.VMEM((2 * tokens, features), bf16),
            pltpu.VMEM((share, features), bf16),
            pltpu.VMEM((share, features), bf16),
            pltpu.VMEM((2 * tokens, features), bf16),
            pltpu.VMEM((2 * tokens, main + extra), bf16),
            pltpu.VMEM((2 * share, features), bf16),
            pltpu.VMEM((share, features), bf16),
            pltpu.VMEM((share, features), bf16),
            pltpu.VMEM(wol.shape, bf16),
            pltpu.VMEM(wob.shape, bf16),
            pltpu.VMEM(residual_in.shape, bf16),
            dma((n_sp,)),
            dma((2,)),
            dma((n_sp,)),
            dma((4, n_sp)),
            dma((4,)),
            dma((10,)),
            dma((12,)),
            dma((12,)),
        ],
        compiler_params=pltpu.CompilerParams(
            collective_id=0, has_side_effects=True, vmem_limit_bytes=62 * 2**20
        ),
    )(*args)


def fits(grid, mesh, args):
    if grid is None or mesh.shape["tp"] != 2 or grid[1] != 2 or grid[2] != 2 or grid[0] not in (2, 4, 6, 8):
        return False
    n_sp = mesh.shape["sp"]
    tokens = args[1].shape[0] // n_sp
    share = tokens // 2
    units = args[14].shape[1] // 2
    heads_l, heads_b = args[6].shape[1] // 2, args[7].shape[1] // 2
    wide_l, wide_b = args[6].shape[2], args[7].shape[2]
    rope = args[4].shape[1]
    return (
        tokens % 128 == 0 and tokens <= 256 and share % 16 == 0 and units >= 384
        and units % 256 == 128 and heads_l % 2 == 0 and 2 * wide_l == wide_b and wide_b % 128 == 0
        and args[3].shape[1] == tokens and rope % 32 == 0 and (tokens + rope) % 32 == 0
        and heads_b > 0 and args[8].shape[2] == wide_l and args[9].shape[2] == wide_b
        and args[14].shape[0] // n_sp == 128 and args[16].shape[1] // n_sp == 128
    )


def solution(mesh):
    in_specs = (
        P(("sp", "tp"), None),
        P("sp", "tp", None),
        P("sp", "tp", None),
        P("sp", None),
        P("sp", None),
        P(),
        P(None, "tp", None),
        P(None, "tp", None),
        P(None, "tp", None),
        P(None, "tp", None),
        P("tp", None, None),
        P("tp", None, None),
        P(),
        P(),
        P("sp", "tp"),
        P("sp", "tp"),
        P("tp", "sp"),
    )
    out_specs = P(("sp", "tp"), None)
    grid = grid_of(mesh)

    def layer(*args):
        body = functools.partial(fused_shards, grid) if fits(grid, mesh, args) else shards
        return jax.shard_map(
            body, mesh=mesh, in_specs=in_specs, out_specs=out_specs, check_vma=False
        )(*args)

    return layer
```

```python
import functools
import math

import jax
import jax.numpy as jnp
from jax import lax
from jax.experimental import pallas as pl
from jax.experimental.pallas import tpu as pltpu
from jax.sharding import PartitionSpec as P

THETA = 10000.0
EPS = 1e-06
NEGATIVE = -1e30


def rotate(values, positions):
    width = values.shape[-1]
    half = width // 2
    freqs = THETA ** (-2.0 * jnp.arange(half, dtype=jnp.float32) / width)
    angle = positions.astype(jnp.float32)[:, None] * freqs[None, :]
    cosine = jnp.cos(angle)
    sine = jnp.sin(angle)
    if values.ndim == 3:
        cosine = cosine[:, None, :]
        sine = sine[:, None, :]
    first = values[..., :half]
    second = values[..., half:]
    return jnp.concatenate(
        [first * cosine - second * sine, first * sine + second * cosine], axis=-1
    )


def normalize(values, gain):
    return values * lax.rsqrt(jnp.mean(values * values, axis=-1, keepdims=True) + EPS) * gain


def block_keys(weights, latent_rows):
    projected = []
    for key_up, value_up in weights:
        keys = jnp.einsum(
            "kr,rhd->khd", latent_rows, key_up, preferred_element_type=jnp.float32
        ).astype(jnp.bfloat16)
        values = jnp.einsum(
            "kr,rhd->khd", latent_rows, value_up, preferred_element_type=jnp.float32
        ).astype(jnp.bfloat16)
        projected.append((keys, values))
    return projected


def attend(carry, queries, projected, rotated_rows, key_pos, query_pos):
    updated = []
    visible = key_pos[None, :] <= query_pos[:, None]
    for state, query, pair in zip(carry, queries, projected):
        query_nope, query_rot, scale = query
        keys, values = pair
        peak, total, accum = state
        scores = (
            jnp.einsum("qhd,khd->hqk", query_nope, keys, preferred_element_type=jnp.float32)
            + jnp.einsum("qhr,kr->hqk", query_rot, rotated_rows, preferred_element_type=jnp.float32)
        ) * scale
        scores = jnp.where(visible[None], scores, NEGATIVE)
        new_peak = jnp.maximum(peak, jnp.max(scores, axis=-1))
        weights = jnp.where(visible[None], jnp.exp(scores - new_peak[..., None]), 0.0)
        factor = jnp.exp(peak - new_peak)
        total = total * factor + jnp.sum(weights, axis=-1)
        accum = accum * factor[..., None] + jnp.einsum(
            "hqk,khv->hqv", weights.astype(jnp.bfloat16), values, preferred_element_type=jnp.float32
        )
        updated.append((new_peak, total, accum))
    return tuple(updated)


def fold_piece(carry, latent_piece, rotated_piece, piece_pos, weights, segments):
    count = latent_piece.shape[0]
    block = math.gcd(count, 1024)
    last_all = segments[0][1][-1]

    def one_block(index, state):
        lat_rows = lax.dynamic_slice_in_dim(latent_piece, index * block, block, 0)
        rot_rows = lax.dynamic_slice_in_dim(rotated_piece, index * block, block, 0)
        pos_rows = lax.dynamic_slice_in_dim(piece_pos, index * block, block, 0)
        first_key = jnp.min(pos_rows)

        def work(inner):
            projected = block_keys(weights, lat_rows)
            results = []
            for inner_seg, segment in zip(inner, segments):
                queries, seg_pos = segment
                results.append(
                    lax.cond(
                        first_key <= seg_pos[-1],
                        lambda held, queries=queries, seg_pos=seg_pos: attend(
                            held, queries, projected, rot_rows, pos_rows, seg_pos
                        ),
                        lambda held: held,
                        inner_seg,
                    )
                )
            return tuple(results)

        return lax.cond(first_key <= last_all, work, lambda inner: inner, state)

    return lax.fori_loop(0, count // block, one_block, carry)


def shards(
    residual_in,
    query_lean,
    query_broad,
    latent,
    rope_key,
    latent_gain,
    key_up_lean,
    key_up_broad,
    value_up_lean,
    value_up_broad,
    out_lean,
    out_broad,
    attn_gain,
    mlp_gain,
    gate_weight,
    up_weight,
    down_weight,
):
    tokens_here = query_lean.shape[0]
    n_tp = lax.axis_size("tp")
    share = tokens_here // n_tp
    sp_index = lax.axis_index("sp")
    first = sp_index * tokens_here
    query_pos = first + jnp.arange(tokens_here, dtype=jnp.int32)
    rope_width = rope_key.shape[1]
    weights = ((key_up_lean, value_up_lean), (key_up_broad, value_up_broad))
    segment_rows = (query_lean, query_broad, query_pos)
    segments = []
    initial = []
    lean_rows, broad_rows, seg_pos = segment_rows
    queries = []
    states = []
    for query, value_up in ((lean_rows, value_up_lean), (broad_rows, value_up_broad)):
        nope = query.shape[2] - rope_width
        query_rot = rotate(query[:, :, nope:].astype(jnp.float32), seg_pos).astype(jnp.bfloat16)
        queries.append((query[:, :, :nope], query_rot, query.shape[2] ** (-0.5)))
        heads = query.shape[1]
        rows = query.shape[0]
        states.append(
            (
                jnp.full((heads, rows), NEGATIVE, jnp.float32),
                jnp.zeros((heads, rows), jnp.float32),
                jnp.zeros((heads, rows, value_up.shape[2]), jnp.float32),
            )
        )
    segments.append((tuple(queries), seg_pos))
    initial.append(tuple(states))
    segments = tuple(segments)
    initial = tuple(initial)
    sent_latent = normalize(latent.astype(jnp.float32), latent_gain).astype(jnp.bfloat16)
    sent_rot = rotate(rope_key.astype(jnp.float32), query_pos).astype(jnp.bfloat16)
    pieces = (
        lax.all_gather(sent_latent, "sp", axis=0, tiled=True),
        lax.all_gather(sent_rot, "sp", axis=0, tiled=True),
    )
    piece_pos = jnp.arange(pieces[0].shape[0], dtype=jnp.int32)
    folded = fold_piece(initial, pieces[0], pieces[1], piece_pos, weights, segments)
    results = [
        [(accum / total[..., None]).astype(jnp.bfloat16) for peak, total, accum in seg_state]
        for seg_state in folded
    ]
    attended = results[0]
    term = jnp.zeros((share * lax.axis_size("tp"), out_lean.shape[2]), jnp.float32)
    for rows_all, weight in ((attended[0], out_lean), (attended[1], out_broad)):
        rows = rows_all
        term = term + jnp.einsum("hqv,hvd->qd", rows, weight, preferred_element_type=jnp.float32)
    head_sum = lax.psum_scatter(
        term.astype(jnp.bfloat16), "tp", scatter_dimension=0, tiled=True
    ).astype(jnp.float32)
    branch = normalize(head_sum, attn_gain)
    kept = (residual_in.astype(jnp.float32) + branch).astype(jnp.bfloat16)
    normed = normalize(kept.astype(jnp.float32), mlp_gain).astype(jnp.bfloat16)
    whole_normed = lax.all_gather(normed, "tp", axis=0, tiled=True)
    gate_whole, up_whole, down_whole = (
        lax.all_gather(gate_weight, "sp", axis=0, tiled=True),
        lax.all_gather(up_weight, "sp", axis=0, tiled=True),
        lax.all_gather(down_weight, "sp", axis=1, tiled=True),
    )
    gate = jnp.dot(whole_normed, gate_whole, preferred_element_type=jnp.float32)
    up = jnp.dot(whole_normed, up_whole, preferred_element_type=jnp.float32)
    hidden = (jax.nn.silu(gate) * up).astype(jnp.bfloat16)
    rows = hidden
    channel_sum = lax.psum_scatter(
        jnp.dot(rows, down_whole, preferred_element_type=jnp.float32).astype(jnp.bfloat16),
        "tp",
        scatter_dimension=0,
        tiled=True,
    ).astype(jnp.float32)
    return (kept.astype(jnp.float32) + 0.5 * channel_sum).astype(jnp.bfloat16)


LOG2E = math.log2(math.e)


def grid_of(mesh):
    n_sp, n_tp = mesh.shape["sp"], mesh.shape["tp"]
    devices = mesh.devices.reshape(n_sp, n_tp)
    try:
        places = [tuple(device.coords) for device in devices[:, 0]]
        partners = [tuple(device.coords) for device in devices[:, -1]]
    except Exception:
        return (n_sp // 4, 2, 2) if n_sp % 4 == 0 else None
    if places != partners:
        return None
    low = [min(place[k] for place in places) for k in range(3)]
    sizes = [max(place[k] for place in places) - low[k] + 1 for k in range(3)]
    wide_z, wide_y, wide_x = sizes[2], sizes[1], sizes[0]
    if wide_z * wide_y * wide_x != n_sp:
        return None
    for index, place in enumerate(places):
        x, y, z = (place[k] - low[k] for k in range(3))
        if (z * wide_y + y) * wide_x + x != index:
            return None
    return wide_z, wide_y, wide_x


def hop_table(grid):
    wide_z = grid[0]
    entries = [
        (dz, fy, fx)
        for dz in range(1 - wide_z, wide_z)
        for fy in range(2)
        for fx in range(2)
        if (dz, fy, fx) != (0, 0, 0)
    ]
    entries.sort(key=lambda e: (abs(e[0]) + e[1] + e[2], abs(e[0]), e))
    return entries


def layer_kernel(
    grid, shapes, res_in, qlt, qbt, lat_in, rope_in, lg, ag, mg, kul, kub_in, vul, vub_in, wol_in, wob_in, gw, uw, dw, out,
    lat, kub, vub, cosine, sine, lat_all, gate_all, up_all, down_all, ext_all, own_g, own_u, own_d, own_e, ql, qb, keyn, scores, weigh, valt_l, valt_b,
    peak, total, acc_l, acc_b, att, term, inbox, kept, rows_all, hidden, inbox2, psum, inbox3, wol, wob, res,
    lat_recv, lat_send, lat_pair, recv, send, own_sem, pair_send, pair_recv,
):
    wide_z, wide_y, wide_x = grid
    n_sp = wide_z * wide_y * wide_x
    tokens, share, rope = shapes
    heads_l, heads_b = qlt.shape[0], qbt.shape[0]
    bf16, f32 = jnp.bfloat16, jnp.float32
    me = lax.axis_index("sp")
    core = lax.axis_index("tp")
    my_x = lax.rem(me, wide_x)
    my_y = lax.rem(me // wide_x, wide_y)
    my_z = me // (wide_x * wide_y)
    layer = wide_y * wide_x
    flip_y = me + (1 - 2 * my_y) * wide_x
    flip_x = me + (1 - 2 * my_x)
    side = lax.rem(my_z, 2)
    partner = me + (1 - 2 * side) * layer
    z_ways = [
        (step, my_z + step < wide_z if step > 0 else my_z + step >= 0,
         jnp.clip(me + step * layer, 0, n_sp - 1))
        for step in (1, -1, 2, -2, 3, -3)
    ]

    def z_way(step):
        return next(way for way in z_ways if way[0] == step)

    def run(condition, action):
        pl.when(condition)(action)

    gate_rows, units = gw.shape
    down_cols = dw.shape[1]
    extra = ext_all.shape[2]
    main = (units - extra) // 2
    fetch = [
        pltpu.make_async_copy(src, dst, own_sem.at[k])
        for k, (src, dst) in enumerate((
            (gw, own_g), (uw, own_u), (dw, own_d),
            (gw.at[:, pl.ds(2 * main, extra)], own_e.at[0]),
            (uw.at[:, pl.ds(2 * main, extra)], own_e.at[1]),
            (dw.at[pl.ds(2 * main, extra), :], own_e.at[2]),
            (wol_in, wol), (wob_in, wob), (res_in, res),
        ))
    ]
    for copy in fetch:
        copy.start()
    half_rope = rope // 2
    lane = lax.broadcasted_iota(jnp.int32, (half_rope, tokens), 1)
    line = lax.broadcasted_iota(jnp.int32, (half_rope, tokens), 0)
    freqs = jnp.zeros((half_rope, tokens), f32)
    for k in range(half_rope):
        freqs = jnp.where(line == k, THETA ** (-2.0 * k / rope), freqs)
    angle = (me * tokens + lane).astype(f32) * freqs
    cosine[...] = jnp.cos(angle)
    sine[...] = jnp.sin(angle)
    lat[:tokens, :] = normalize(lat_in[...].astype(f32), lg[...]).astype(bf16)
    one, two = rope_in[:half_rope, :].astype(f32), rope_in[half_rope:, :].astype(f32)
    lat[tokens:tokens + half_rope, :] = (one * cosine[...] - two * sine[...]).astype(bf16)
    lat[tokens + half_rope:, :] = (one * sine[...] + two * cosine[...]).astype(bf16)
    lat_rows = lat.shape[0]
    barrier = pltpu.get_barrier_semaphore()
    for where in (flip_x, flip_y):
        pl.semaphore_signal(barrier, inc=1, device_id={"sp": where})
    pl.semaphore_signal(barrier, inc=1, device_id={"tp": 1 - core})
    greeted = 3
    for _, exists, where in z_ways:
        run(exists, lambda where=where: pl.semaphore_signal(barrier, inc=1, device_id={"sp": where}))
        greeted = greeted + jnp.where(exists, 1, 0)
    pl.semaphore_wait(barrier, greeted)

    half = lat_rows // 2
    first = pl.multiple_of(core * half, 16)

    def lat_at(i):
        return lat_all.at[pl.ds(pl.multiple_of(i * lat_rows + first, 16), half)]

    def lat_copy(i, mine, where):
        return pltpu.make_async_remote_copy(
            src_ref=lat.at[pl.ds(first, half)] if mine else lat_at(i), dst_ref=lat_at(i),
            send_sem=lat_send.at[0], recv_sem=lat_recv.at[i], device_id={"sp": where},
        )

    def pair_lat(i):
        return pltpu.make_async_remote_copy(
            src_ref=lat_at(i), dst_ref=lat_at(i), send_sem=lat_send.at[1],
            recv_sem=lat_pair.at[i], device_id={"tp": 1 - core},
        )

    turn = jnp.where(core == 0, flip_x, flip_y)
    away = jnp.where(core == 0, flip_y, flip_x)

    def lat_spread(i, mine):
        _, exists, where = z_way(1)
        run(exists, lambda: lat_copy(i, mine, where).start())
        lat_copy(i, mine, turn).start()
        lat_copy(i, mine, away).start()

    lat_spread(me, True)

    per = 4

    def words_of(table):
        codes = [((dz + wide_z - 1) * 2 + fy) * 2 + fx for dz, fy, fx in table]
        return [
            sum(code << (7 * k) for k, code in enumerate(codes[at:at + per]))
            for at in range(0, len(codes), per)
        ]

    def origin_of(n, words):
        word = jnp.int32(words[0])
        for k in range(1, len(words)):
            word = jnp.where(n // per == k, jnp.int32(words[k]), word)
        rem = lax.rem(n, per)
        for k in range(1, per):
            word = jnp.where(rem >= k, word // 128, word)
        code = lax.rem(word, 128)
        return code // 4 - (wide_z - 1), lax.rem(code // 2, 2), lax.rem(code, 2)

    def index_of(dz, fy, fx):
        oy = my_y + fy * (1 - 2 * my_y)
        ox = my_x + fx * (1 - 2 * my_x)
        return ((my_z + dz) * wide_y + oy) * wide_x + ox

    def lat_event(dz, fy, fx, column, line):
        i = index_of(dz, fy, fx)
        lat_copy(i, False, turn).wait_recv()
        if column:
            lat_spread(i, False)
        if line:
            lat_copy(i, False, away).start()
        pair_lat(i).start()

    def lat_column(down):
        run(my_z >= down, lambda: lat_event(-down, 0, 0, True, False))

    def lat_side(down):
        def events_of():
            near = jnp.where(core == 0, 0, 1)
            lat_event(-down, near, 1 - near, False, True)
            lat_event(-down, 1 - near, near, False, False)

        run(my_z >= down, events_of)

    def lat_far(down):
        run(my_z >= down, lambda: lat_event(-down, 1, 1, False, False))

    def slot_at(ref, i):
        return ref.at[pl.ds(pl.multiple_of(i * gate_rows, gate_rows), gate_rows), pl.ds(0, main)]

    def down_slot(dz, fy, fx):
        slot = (fy * 2 + fx) * wide_z + my_z + dz
        return down_all.at[pl.ds(0, main), pl.ds(pl.multiple_of(slot * down_cols, down_cols), down_cols)]

    def place(p, dz, fy, fx):
        i = index_of(dz, fy, fx)
        if p == 0:
            return slot_at(gate_all, i)
        if p == 1:
            return slot_at(up_all, i)
        if p == 2:
            return down_slot(dz, fy, fx)
        return ext_all.at[i]

    def own_half(p, h):
        lanes = pl.ds(pl.multiple_of(h * main, extra), main)
        if p == 0:
            return own_g.at[:, lanes]
        if p == 1:
            return own_u.at[:, lanes]
        if p == 2:
            return own_d.at[lanes, :]
        return own_e

    def part_copy(p, src, dst, i, where):
        return pltpu.make_async_remote_copy(
            src_ref=src, dst_ref=dst, send_sem=send.at[p], recv_sem=recv.at[p, i], device_id={"sp": where},
        )

    has_extra = core == side

    def to_z(p, src, step, origin, i, condition=True):
        _, exists, where = z_way(step)
        dst = place(p, *origin) if p == 2 else place(p, *origin)
        run(jnp.logical_and(exists, condition), lambda: part_copy(p, src, dst, i, where).start())

    def seen(origin, fy, fx):
        return origin[0], origin[1] + fy - 2 * origin[1] * fy, origin[2] + fx - 2 * origin[2] * fx

    def dst_for(p, origin, fy, fx):
        if p == 2:
            return down_slot(*seen(origin, fy, fx))
        return place(p, *origin)

    def send_own(p, steps, in_layer, when=True):
        here = (0, 0, 0)
        mine = own_half(p, side)
        other = own_half(p, 1 - side)
        same = has_extra if p == 3 else True
        cross = jnp.logical_not(has_extra) if p == 3 else True
        for step in steps:
            if step % 2:
                to_z(p, other, step, here, me, jnp.logical_and(cross, when))
            else:
                to_z(p, mine, step, here, me, jnp.logical_and(same, when))

        def flips():
            part_copy(p, mine, dst_for(p, here, 0, 1), me, flip_x).start()
            part_copy(p, mine, dst_for(p, here, 1, 0), me, flip_y).start()

        if in_layer and p == 3:
            run(has_extra, flips)
        elif in_layer:
            flips()

    def part_event(p, dz, fy, fx):
        origin = (dz, fy, fx)
        i = index_of(*origin)
        here = place(p, *origin)
        part_copy(p, here, here, i, flip_x).wait_recv()
        column = jnp.logical_and(fy == 0, fx == 0)
        x_line = jnp.logical_and(fy == 0, fx == 1)
        y_line = jnp.logical_and(fy == 1, fx == 0)
        if p == 0:
            to_x, to_y = column, jnp.logical_or(column, x_line)
        elif p == 1:
            to_x, to_y = jnp.logical_or(column, y_line), column
        else:
            x_first = core == 0 if p == 2 else lax.rem(my_z + dz, 2) == 0
            to_x = jnp.logical_or(column, jnp.logical_and(y_line, jnp.logical_not(x_first)))
            to_y = jnp.logical_or(column, jnp.logical_and(x_line, x_first))
        run(to_x, lambda: part_copy(p, here, dst_for(p, origin, 0, 1), i, flip_x).start())
        run(to_y, lambda: part_copy(p, here, dst_for(p, origin, 1, 0), i, flip_y).start())

    for copy in fetch[:6]:
        copy.wait()
    gates = (0, 1, 3, 2)
    for p in gates:
        send_own(p, (-1, -2, -3), False)
        send_own(p, (1, 2, 3), False, my_z == 0)
    lat_column(1)
    for p in gates:
        send_own(p, (1, 2, 3), False, my_z == 1)
    lat_side(0)
    if wide_z > 2:
        lat_column(2)
        for p in gates:
            send_own(p, (1, 2, 3), False, my_z == 2)
    lat_side(1)
    for p in gates:
        send_own(p, (), True)
    lat_far(0)
    lat_far(1)

    whole = hop_table(grid)
    whole_words = words_of(whole)
    count = len(whole)
    hops = [abs(dz) + fy + fx for dz, fy, fx in whole]
    early = sum(1 for hop in hops if hop <= 2)
    ready = sum(1 for hop in hops if hop < wide_z)
    early = sum(1 for hop in hops if hop <= 2)
    groups = ((0, 0), (0, 1), (1, 0), (1, 1))
    grouped = whole
    grouped_words = words_of(grouped)
    lag = count - ready

    def inside(dz):
        return jnp.logical_and(my_z + dz >= 0, my_z + dz < wide_z)

    def events(low, high):
        def gate_parts(n):
            dz, fy, fx = origin_of(n, whole_words)

            @pl.when(inside(dz))
            def _():
                part_event(0, dz, fy, fx)
                part_event(1, dz, fy, fx)
                run(has_extra, lambda: part_event(3, dz, fy, fx))

        def downs(n):
            dz, fy, fx = origin_of(n, grouped_words)
            run(inside(dz), lambda: part_event(2, dz, fy, fx))

        def body(t, _):
            run(t < count, lambda: gate_parts(t))
            run(t >= lag, lambda: downs(t - lag))
            return 0

        lax.fori_loop(low, high, body, 0)

    own_rows = pl.ds(pl.multiple_of(me * gate_rows, gate_rows), gate_rows)
    own_lanes = pl.ds(pl.multiple_of(side * main, extra), main)
    gate_all[own_rows, :main] = own_g[:, own_lanes]
    up_all[own_rows, :main] = own_u[:, own_lanes]
    down_all[:main, pl.ds(pl.multiple_of(my_z * down_cols, down_cols), down_cols)] = own_d[own_lanes, :]
    ext_all[me] = own_e[...]

    wide_l = kul.shape[0] // heads_l
    wide_b = kub.shape[1] // heads_b
    for h in range(heads_b):
        part = slice(h * wide_b, (h + 1) * wide_b)
        kub[:, part] = kub_in[:, h, :]
        vub[part, :] = vub_in[:, h, :].T
    for given, query in ((qlt, ql), (qbt, qb)):
        nope = given.shape[1] - rope
        for h in range(given.shape[0]):
            one = given[h, nope:nope + half_rope, :].astype(f32)
            two = given[h, nope + half_rope:, :].astype(f32)
            if nope < wide_b:
                query[h, :wide_b, :] = jnp.zeros((wide_b, tokens), bf16)
            at = (h * nope) % wide_b
            query[h, at:at + nope, :] = given[h, :nope, :]
            query[h, wide_b:wide_b + half_rope, :] = (one * cosine[...] - two * sine[...]).astype(bf16)
            query[h, wide_b + half_rope:, :] = (one * sine[...] + two * cosine[...]).astype(bf16)
    lat_all[pl.ds(pl.multiple_of(me * lat_rows, 16), lat_rows), :] = lat[...]

    peak[...] = jnp.full(peak.shape, NEGATIVE, f32)
    total[...] = jnp.zeros(total.shape, f32)
    acc_l[...] = jnp.zeros(acc_l.shape, f32)
    acc_b[...] = jnp.zeros(acc_b.shape, f32)
    contract = (((1,), (1,)), ((), ()))
    strip = math.gcd(tokens, 64)
    strips = [slice(at, at + strip) for at in range(0, tokens, strip)]

    def attend_block(j, masked):
        at_j = pl.multiple_of(j * lat_rows, 16)
        rows = lat_all[pl.ds(at_j, tokens), :]
        rot = lat_all[pl.ds(pl.multiple_of(at_j + tokens, 16), rope), :].T
        split = heads_l * wide_l
        keyn[:, :split] = lax.dot_general(rows, kul[...], contract, preferred_element_type=f32).astype(bf16)
        keyn[:, split:] = jnp.dot(rows, kub[...], preferred_element_type=f32).astype(bf16)
        for ups, held in ((vul, valt_l), (vub, valt_b)):
            held[...] = lax.dot_general(
                ups[...], rows, contract, preferred_element_type=f32
            ).astype(bf16)

        def of(g):
            if g < heads_l:
                return g, ql, valt_l, acc_l, wide_l, wide_l + rope
            return g - heads_l, qb, valt_b, acc_b, wide_b, wide_b + rope

        def score(g):
            h, query = of(g)[:2]
            at = (g * wide_l // wide_b if g < heads_l else split // wide_b + h) * wide_b
            keys = jnp.concatenate([keyn[:, at:at + wide_b], rot], axis=1)
            held = jnp.dot(keys, query[h], preferred_element_type=f32)
            if masked:
                key_pos = lax.broadcasted_iota(jnp.int32, (tokens, tokens), 0)
                visible = key_pos <= lax.broadcasted_iota(jnp.int32, (tokens, tokens), 1)
                held = jnp.where(visible, held, NEGATIVE)
            scores[g % 2] = held

        score(0)
        for g in range(heads_l + heads_b):
            if g + 1 < heads_l + heads_b:
                score(g + 1)
            h, query, held, acc, wide, size = of(g)
            scale = LOG2E * size ** (-0.5)
            old = peak[g]
            top = jnp.max(scores[g % 2, strips[0], :], axis=0, keepdims=True)
            for part in strips[1:]:
                top = jnp.maximum(top, jnp.max(scores[g % 2, part, :], axis=0, keepdims=True))
            new = jnp.maximum(old, top * scale)
            factor = jnp.exp2(old - new)
            summed = total[g] * factor
            for part in strips:
                weights = jnp.exp2(scores[g % 2, part, :] * scale - new)
                summed = summed + jnp.sum(weights, axis=0, keepdims=True)
                weigh[g % 2, part, :] = weights.astype(bf16)
            peak[g] = new
            total[g] = summed
            acc[h] = acc[h] * factor + jnp.dot(
                held[h * wide:(h + 1) * wide, :], weigh[g % 2], preferred_element_type=f32
            )

    def attend_layer(down, low, high):
        def body(t, _):
            events(low + (t * (high - low)) // layer, low + ((t + 1) * (high - low)) // layer)
            i = (my_z - down) * layer + t

            @pl.when(jnp.logical_and(my_z >= down, i < me))
            def _():
                pair_lat(i).wait_recv()
                attend_block(i, False)

            return 0

        lax.fori_loop(0, layer, body, 0)

    attend_block(me, True)
    attend_layer(0, 0, 0)
    for down in range(1, wide_z):
        if down == 1 and wide_z > 2:
            lat_column(3)
            lat_side(2)
            lat_far(2)
        if down == 2:
            lat_side(3)
            lat_far(3)
        attend_layer(down, (down - 1) * early // (wide_z - 1), down * early // (wide_z - 1))

    def rest(i, _):
        run(jnp.logical_and(i > me, i < (my_z + 1) * layer), lambda: pair_lat(i).wait_recv())
        return 0

    lax.fori_loop(0, n_sp, rest, 0)

    split = heads_l * wide_l
    for heads, wide, acc, base, col in (
        (heads_l, wide_l, acc_l, 0, 0), (heads_b, wide_b, acc_b, heads_l, split),
    ):
        together = wide_b // wide
        for h in range(0, heads, together):
            done = jnp.concatenate(
                [acc[h + k] / total[base + h + k] for k in range(together)], axis=0
            )
            att[:, col + h * wide:col + (h + together) * wide] = done.T.astype(bf16)

    features = out.shape[1]
    block = math.gcd(features, 512)

    for copy in fetch[6:]:
        copy.wait()

    def project(n, _):
        cols = pl.ds(pl.multiple_of(n * block, block), block)
        term[:tokens, cols] = (
            jnp.dot(att[:, :split], wol[:, cols], preferred_element_type=f32)
            + jnp.dot(att[:, split:], wob[:, cols], preferred_element_type=f32)
        ).astype(bf16)
        return 0

    lax.fori_loop(0, features // block, project, 0)
    theirs = pl.ds(pl.multiple_of((1 - core) * share, share), share)

    def to_pair(k, src, dst):
        return pltpu.make_async_remote_copy(
            src_ref=src, dst_ref=dst, send_sem=pair_send.at[k], recv_sem=pair_recv.at[k],
            device_id={"tp": 1 - core},
        )

    def to_partner(k, src, dst):
        return pltpu.make_async_remote_copy(
            src_ref=src, dst_ref=dst, send_sem=pair_send.at[k], recv_sem=pair_recv.at[k],
            device_id={"sp": partner},
        )

    def place_of(of_core, of_side):
        return pl.ds(pl.multiple_of((of_side * 2 + of_core) * share, share), share)

    heads_out = to_pair(0, term.at[theirs], inbox)
    heads_out.start()
    heads_out.wait_recv()
    rows_at_once = math.gcd(share, 16)

    def norms(n, _):
        rows = pl.ds(pl.multiple_of(n * rows_at_once, rows_at_once), rows_at_once)
        full = pl.ds(pl.multiple_of(core * share + n * rows_at_once, rows_at_once), rows_at_once)
        spot = pl.ds(pl.multiple_of((side * 2 + core) * share + n * rows_at_once, rows_at_once), rows_at_once)
        summed = term[full, :].astype(f32) + inbox[rows, :].astype(f32)
        branch = normalize(summed, ag[...])
        mixed = (res[rows, :].astype(f32) + branch).astype(bf16)
        kept[rows, :] = mixed
        rows_all[spot, :] = normalize(mixed.astype(f32), mg[...]).astype(bf16)
        return 0

    lax.fori_loop(0, share // rows_at_once, norms, 0)
    mine_at = rows_all.at[place_of(core, side)]
    rows_out = to_pair(1, mine_at, mine_at)
    rows_far = to_partner(2, mine_at, mine_at)
    rows_out.start()
    rows_far.start()
    heads_out.wait_send()
    ready = sum(1 for hop in hops if hop < wide_z)
    events(early, ready)
    far_at = rows_all.at[place_of(core, 1 - side)]
    to_partner(2, far_at, far_at).wait_recv()
    rows_on = to_pair(3, far_at, far_at)
    rows_on.start()
    near_at = rows_all.at[place_of(1 - core, side)]
    to_pair(1, near_at, near_at).wait_recv()
    last_at = rows_all.at[place_of(1 - core, 1 - side)]
    to_pair(3, last_at, last_at).wait_recv()
    events(ready, count)

    def feed_from(rows, gate_w, up_w, cols):
        gate = jnp.dot(rows_all[rows, :], gate_w, preferred_element_type=f32)
        up = jnp.dot(rows_all[rows, :], up_w, preferred_element_type=f32)
        hidden[rows, cols] = (gate / (1.0 + jnp.exp(-gate)) * up).astype(bf16)

    span = 256
    chunks = main // span
    group = tokens

    def group_rows(n):
        of_side = jnp.where(n == 0, 1 - side, side)
        return pl.ds(pl.multiple_of(of_side * group, group), group)

    @pl.when(has_extra)
    def _():
        def lay(i, _):
            oz = i // layer
            fy = jnp.abs(lax.rem(i // wide_x, wide_y) - my_y)
            fx = jnp.abs(lax.rem(i, wide_x) - my_x)
            slot = (fy * 2 + fx) * wide_z + oz
            at_i = pl.ds(pl.multiple_of(i * gate_rows, gate_rows), gate_rows)
            gate_all[at_i, main:] = ext_all[i, 0]
            up_all[at_i, main:] = ext_all[i, 1]
            down_all[main:, pl.ds(pl.multiple_of(slot * down_cols, down_cols), down_cols)] = ext_all[i, 2]
            return 0

        lax.fori_loop(0, n_sp, lay, 0)

    def feed(half):
        rows = group_rows(half)

        def body(n, _):
            cols = pl.ds(pl.multiple_of(n * span, span), span)
            feed_from(rows, gate_all[:, cols], up_all[:, cols], cols)
            return 0

        lax.fori_loop(0, chunks, body, 0)

        def rest(high):
            cols = slice(chunks * span, high)
            if high > chunks * span:
                feed_from(rows, gate_all[:, cols], up_all[:, cols], cols)

        run(has_extra, lambda: rest(main + extra))
        run(jnp.logical_not(has_extra), lambda: rest(main))

    wide_k = wide_z * down_cols
    wide_n = math.gcd(wide_k, 256)
    pieces = wide_k // wide_n

    def down_with(depth, half, low, high):
        rows = group_rows(half)

        def body(n, _):
            cols = pl.ds(pl.multiple_of(n * wide_n, wide_n), wide_n)
            term[rows, cols] = jnp.dot(
                hidden[rows, :depth], down_all[:depth, cols], preferred_element_type=f32
            ).astype(bf16)
            return 0

        lax.fori_loop(low * pieces, high * pieces, body, 0)

    def down(half, low, high):
        run(has_extra, lambda: down_with(main + extra, half, low, high))
        run(jnp.logical_not(has_extra), lambda: down_with(main, half, low, high))

    sums, sums_far = [], []

    def pair_sums(k):
        cols = pl.ds(k * wide_k, wide_k)
        sums.append(to_pair(4 + k, term.at[place_of(1 - core, 1 - side), cols], inbox2.at[pl.ds(0, share), cols]))
        sums[k].start()

    def far_sums(k):
        cols = pl.ds(k * wide_k, wide_k)
        sums[k].wait_recv()
        psum[:, cols] = (
            term[place_of(core, 1 - side), cols].astype(f32) + inbox2[:share, cols].astype(f32)
        ).astype(bf16)
        sums_far.append(to_partner(8 + k, psum.at[:, cols], inbox3.at[:, cols]))
        sums_far[k].start()

    feed(0)
    since = count
    for k, (fy, fx) in enumerate(groups):
        until = lag + max(n + 1 for n, e in enumerate(grouped) if e[1:] == (fy, fx))
        until = max(until, since)
        events(max(since, count), max(until, count))
        since = until
        down(0, k, k + 1)
        pair_sums(k)
        if k:
            far_sums(k - 1)
    far_sums(len(groups) - 1)
    feed(1)
    down(1, 0, len(groups))
    own_sums = to_pair(12, term.at[place_of(1 - core, side)], inbox2.at[pl.ds(share, share)])
    own_sums.start()

    def drain(ref, sem):
        pltpu.make_async_copy(ref, ref, sem).wait()

    for z in range(wide_z):
        @pl.when(my_z == z)
        def _(z=z):
            up = 1 if z + 1 < wide_z else 0
            drain(lat_all.at[pl.ds(0, (up + 3) * (z + 1) * half)], lat_send.at[0])
            drain(lat_all.at[pl.ds(0, (layer * (z + 1) - 1) * half)], lat_send.at[1])
            two = (1 if z + 2 < wide_z else 0) + (1 if z >= 2 else 0)
            odd = sum(1 for step in (1, -1, 3, -3) if 0 <= z + step < wide_z)
            n = two + odd + 3 * wide_z
            drain(gate_all.at[pl.ds(0, n * gate_rows), pl.ds(0, main)], send.at[0])
            drain(up_all.at[pl.ds(0, n * gate_rows), pl.ds(0, main)], send.at[1])
            drain(down_all.at[pl.ds(0, main), pl.ds(0, n * down_cols)], send.at[2])
            run(has_extra, lambda: drain(ext_all.at[pl.ds(0, two + 3 * wide_z)], send.at[3]))
            run(jnp.logical_not(has_extra), lambda: drain(ext_all.at[pl.ds(0, odd)], send.at[3]))

    own_sums.wait_recv()
    for copy in [rows_out, rows_far, rows_on, own_sums] + sums:
        copy.wait_send()

    for k, (fy, fx) in enumerate(groups):
        sums_far[k].wait_recv()

        def finish(t, _, k=k, fy=fy, fx=fx):
            slot = pl.ds(pl.multiple_of((k * wide_z + t) * down_cols, down_cols), down_cols)
            i = (t * wide_y + my_y + fy * (1 - 2 * my_y)) * wide_x + my_x + fx * (1 - 2 * my_x)
            cols = pl.ds(pl.multiple_of(i * down_cols, down_cols), down_cols)
            summed = (
                term[place_of(core, side), slot].astype(f32)
                + inbox2[share:, slot].astype(f32)
                + inbox3[:, slot].astype(f32)
            )
            out[:, cols] = (kept[:, cols].astype(f32) + 0.5 * summed).astype(bf16)
            return 0

        lax.fori_loop(0, wide_z, finish, 0)
    for copy in sums_far:
        copy.wait_send()


def fused_shards(
    grid, residual_in, query_lean, query_broad, latent, rope_key, latent_gain, key_up_lean,
    key_up_broad, value_up_lean, value_up_broad, out_lean, out_broad, attn_gain, mlp_gain,
    gate_weight, up_weight, down_weight,
):
    bf16, f32 = jnp.bfloat16, jnp.float32
    tokens = query_lean.shape[0]
    share, features = residual_in.shape
    rank = latent.shape[1]
    rope = rope_key.shape[1]
    n_sp = lax.axis_size("sp")
    ql, qb = (jnp.transpose(query, (1, 2, 0)) for query in (query_lean, query_broad))
    kul = key_up_lean.reshape(rank, -1).T
    vul = value_up_lean.reshape(rank, -1).T
    wol = out_lean.reshape(-1, features)
    wob = out_broad.reshape(-1, features)
    heads = ql.shape[0] + qb.shape[0]
    wide_all = qb.shape[0] * value_up_broad.shape[2]
    units = gate_weight.shape[1]
    extra = gate_weight.shape[0]
    main = (units - extra) // 2
    wide_b = value_up_broad.shape[2]
    vmem = pl.BlockSpec(memory_space=pltpu.VMEM)
    args = (
        residual_in, ql, qb, latent, rope_key.T, latent_gain[None], attn_gain[None], mlp_gain[None],
        kul, key_up_broad, vul, value_up_broad, wol, wob,
        gate_weight, up_weight, down_weight,
    )
    dma = pltpu.SemaphoreType.DMA
    return pl.pallas_call(
        functools.partial(layer_kernel, grid, (tokens, share, rope)),
        out_shape=jax.ShapeDtypeStruct((share, features), bf16),
        in_specs=[
            pl.BlockSpec(memory_space=pl.ANY) if k in (0, 12, 13, 14, 15, 16) else vmem for k in range(len(args))
        ],
        out_specs=vmem,
        scratch_shapes=[
            pltpu.VMEM((tokens + rope, rank), bf16),
            pltpu.VMEM((rank, wide_all), bf16),
            pltpu.VMEM((wide_all, rank), bf16),
            pltpu.VMEM((rope // 2, tokens), f32),
            pltpu.VMEM((rope // 2, tokens), f32),
            pltpu.VMEM((n_sp * (tokens + rope), rank), bf16),
            pltpu.VMEM((features, main + extra), bf16),
            pltpu.VMEM((features, main + extra), bf16),
            pltpu.VMEM((main + extra, features), bf16),
            pltpu.VMEM((n_sp, 3, extra, extra), bf16),
            pltpu.VMEM(gate_weight.shape, bf16),
            pltpu.VMEM(up_weight.shape, bf16),
            pltpu.VMEM(down_weight.shape, bf16),
            pltpu.VMEM((3, extra, extra), bf16),
            pltpu.VMEM((ql.shape[0],) + qb.shape[1:], bf16),
            pltpu.VMEM(qb.shape, bf16),
            pltpu.VMEM((tokens, kul.shape[0] + wide_all), bf16),
            pltpu.VMEM((2, tokens, tokens), f32),
            pltpu.VMEM((2, tokens, tokens), bf16),
            pltpu.VMEM((vul.shape[0], tokens), bf16),
            pltpu.VMEM((wide_all, tokens), bf16),
            pltpu.VMEM((heads, 1, tokens), f32),
            pltpu.VMEM((heads, 1, tokens), f32),
            pltpu.VMEM((ql.shape[0], value_up_lean.shape[2], tokens), f32),
            pltpu.VMEM((qb.shape[0], wide_b, tokens), f32),
            pltpu.VMEM((tokens, vul.shape[0] + wide_all), bf16),
            pltpu.VMEM((2 * tokens, features), bf16),
            pltpu.VMEM((share, features), bf16),
            pltpu.VMEM((share, features), bf16),
            pltpu.VMEM((2 * tokens, features), bf16),
            pltpu.VMEM((2 * tokens, main + extra), bf16),
            pltpu.VMEM((2 * share, features), bf16),
            pltpu.VMEM((share, features), bf16),
            pltpu.VMEM((share, features), bf16),
            pltpu.VMEM(wol.shape, bf16),
            pltpu.VMEM(wob.shape, bf16),
            pltpu.VMEM(residual_in.shape, bf16),
            dma((n_sp,)),
            dma((2,)),
            dma((n_sp,)),
            dma((4, n_sp)),
            dma((4,)),
            dma((10,)),
            dma((13,)),
            dma((13,)),
        ],
        compiler_params=pltpu.CompilerParams(
            collective_id=0, has_side_effects=True, vmem_limit_bytes=62 * 2**20
        ),
    )(*args)


def fits(grid, mesh, args):
    if grid is None or mesh.shape["tp"] != 2 or grid[1] != 2 or grid[2] != 2 or grid[0] not in (2, 4, 6, 8):
        return False
    n_sp = mesh.shape["sp"]
    tokens = args[1].shape[0] // n_sp
    share = tokens // 2
    units = args[14].shape[1] // 2
    heads_l, heads_b = args[6].shape[1] // 2, args[7].shape[1] // 2
    wide_l, wide_b = args[6].shape[2], args[7].shape[2]
    rope = args[4].shape[1]
    return (
        tokens % 128 == 0 and tokens <= 256 and share % 16 == 0 and units >= 384
        and units % 256 == 128 and heads_l % 2 == 0 and 2 * wide_l == wide_b and wide_b % 128 == 0
        and args[3].shape[1] == tokens and rope % 32 == 0 and (tokens + rope) % 32 == 0
        and heads_b > 0 and args[8].shape[2] == wide_l and args[9].shape[2] == wide_b
        and args[14].shape[0] // n_sp == 128 and args[16].shape[1] // n_sp == 128
    )


def solution(mesh):
    in_specs = (
        P(("sp", "tp"), None),
        P("sp", "tp", None),
        P("sp", "tp", None),
        P("sp", None),
        P("sp", None),
        P(),
        P(None, "tp", None),
        P(None, "tp", None),
        P(None, "tp", None),
        P(None, "tp", None),
        P("tp", None, None),
        P("tp", None, None),
        P(),
        P(),
        P("sp", "tp"),
        P("sp", "tp"),
        P("tp", "sp"),
    )
    out_specs = P(("sp", "tp"), None)
    grid = grid_of(mesh)

    def layer(*args):
        body = functools.partial(fused_shards, grid) if fits(grid, mesh, args) else shards
        return jax.shard_map(
            body, mesh=mesh, in_specs=in_specs, out_specs=out_specs, check_vma=False
        )(*args)

    return layer
```

```python
import functools
import math

import jax
import jax.numpy as jnp
from jax import lax
from jax.experimental import pallas as pl
from jax.experimental.pallas import tpu as pltpu
from jax.sharding import PartitionSpec as P

THETA = 10000.0
EPS = 1e-06
NEGATIVE = -1e30


def rotate(values, positions):
    width = values.shape[-1]
    half = width // 2
    freqs = THETA ** (-2.0 * jnp.arange(half, dtype=jnp.float32) / width)
    angle = positions.astype(jnp.float32)[:, None] * freqs[None, :]
    cosine = jnp.cos(angle)
    sine = jnp.sin(angle)
    if values.ndim == 3:
        cosine = cosine[:, None, :]
        sine = sine[:, None, :]
    first = values[..., :half]
    second = values[..., half:]
    return jnp.concatenate(
        [first * cosine - second * sine, first * sine + second * cosine], axis=-1
    )


def normalize(values, gain):
    return values * lax.rsqrt(jnp.mean(values * values, axis=-1, keepdims=True) + EPS) * gain


def block_keys(weights, latent_rows):
    projected = []
    for key_up, value_up in weights:
        keys = jnp.einsum(
            "kr,rhd->khd", latent_rows, key_up, preferred_element_type=jnp.float32
        ).astype(jnp.bfloat16)
        values = jnp.einsum(
            "kr,rhd->khd", latent_rows, value_up, preferred_element_type=jnp.float32
        ).astype(jnp.bfloat16)
        projected.append((keys, values))
    return projected


def attend(carry, queries, projected, rotated_rows, key_pos, query_pos):
    updated = []
    visible = key_pos[None, :] <= query_pos[:, None]
    for state, query, pair in zip(carry, queries, projected):
        query_nope, query_rot, scale = query
        keys, values = pair
        peak, total, accum = state
        scores = (
            jnp.einsum("qhd,khd->hqk", query_nope, keys, preferred_element_type=jnp.float32)
            + jnp.einsum("qhr,kr->hqk", query_rot, rotated_rows, preferred_element_type=jnp.float32)
        ) * scale
        scores = jnp.where(visible[None], scores, NEGATIVE)
        new_peak = jnp.maximum(peak, jnp.max(scores, axis=-1))
        weights = jnp.where(visible[None], jnp.exp(scores - new_peak[..., None]), 0.0)
        factor = jnp.exp(peak - new_peak)
        total = total * factor + jnp.sum(weights, axis=-1)
        accum = accum * factor[..., None] + jnp.einsum(
            "hqk,khv->hqv", weights.astype(jnp.bfloat16), values, preferred_element_type=jnp.float32
        )
        updated.append((new_peak, total, accum))
    return tuple(updated)


def fold_piece(carry, latent_piece, rotated_piece, piece_pos, weights, segments):
    count = latent_piece.shape[0]
    block = math.gcd(count, 1024)
    last_all = segments[0][1][-1]

    def one_block(index, state):
        lat_rows = lax.dynamic_slice_in_dim(latent_piece, index * block, block, 0)
        rot_rows = lax.dynamic_slice_in_dim(rotated_piece, index * block, block, 0)
        pos_rows = lax.dynamic_slice_in_dim(piece_pos, index * block, block, 0)
        first_key = jnp.min(pos_rows)

        def work(inner):
            projected = block_keys(weights, lat_rows)
            results = []
            for inner_seg, segment in zip(inner, segments):
                queries, seg_pos = segment
                results.append(
                    lax.cond(
                        first_key <= seg_pos[-1],
                        lambda held, queries=queries, seg_pos=seg_pos: attend(
                            held, queries, projected, rot_rows, pos_rows, seg_pos
                        ),
                        lambda held: held,
                        inner_seg,
                    )
                )
            return tuple(results)

        return lax.cond(first_key <= last_all, work, lambda inner: inner, state)

    return lax.fori_loop(0, count // block, one_block, carry)


def shards(
    residual_in,
    query_lean,
    query_broad,
    latent,
    rope_key,
    latent_gain,
    key_up_lean,
    key_up_broad,
    value_up_lean,
    value_up_broad,
    out_lean,
    out_broad,
    attn_gain,
    mlp_gain,
    gate_weight,
    up_weight,
    down_weight,
):
    tokens_here = query_lean.shape[0]
    n_tp = lax.axis_size("tp")
    share = tokens_here // n_tp
    sp_index = lax.axis_index("sp")
    first = sp_index * tokens_here
    query_pos = first + jnp.arange(tokens_here, dtype=jnp.int32)
    rope_width = rope_key.shape[1]
    weights = ((key_up_lean, value_up_lean), (key_up_broad, value_up_broad))
    segment_rows = (query_lean, query_broad, query_pos)
    segments = []
    initial = []
    lean_rows, broad_rows, seg_pos = segment_rows
    queries = []
    states = []
    for query, value_up in ((lean_rows, value_up_lean), (broad_rows, value_up_broad)):
        nope = query.shape[2] - rope_width
        query_rot = rotate(query[:, :, nope:].astype(jnp.float32), seg_pos).astype(jnp.bfloat16)
        queries.append((query[:, :, :nope], query_rot, query.shape[2] ** (-0.5)))
        heads = query.shape[1]
        rows = query.shape[0]
        states.append(
            (
                jnp.full((heads, rows), NEGATIVE, jnp.float32),
                jnp.zeros((heads, rows), jnp.float32),
                jnp.zeros((heads, rows, value_up.shape[2]), jnp.float32),
            )
        )
    segments.append((tuple(queries), seg_pos))
    initial.append(tuple(states))
    segments = tuple(segments)
    initial = tuple(initial)
    sent_latent = normalize(latent.astype(jnp.float32), latent_gain).astype(jnp.bfloat16)
    sent_rot = rotate(rope_key.astype(jnp.float32), query_pos).astype(jnp.bfloat16)
    pieces = (
        lax.all_gather(sent_latent, "sp", axis=0, tiled=True),
        lax.all_gather(sent_rot, "sp", axis=0, tiled=True),
    )
    piece_pos = jnp.arange(pieces[0].shape[0], dtype=jnp.int32)
    folded = fold_piece(initial, pieces[0], pieces[1], piece_pos, weights, segments)
    results = [
        [(accum / total[..., None]).astype(jnp.bfloat16) for peak, total, accum in seg_state]
        for seg_state in folded
    ]
    attended = results[0]
    term = jnp.zeros((share * lax.axis_size("tp"), out_lean.shape[2]), jnp.float32)
    for rows_all, weight in ((attended[0], out_lean), (attended[1], out_broad)):
        rows = rows_all
        term = term + jnp.einsum("hqv,hvd->qd", rows, weight, preferred_element_type=jnp.float32)
    head_sum = lax.psum_scatter(
        term.astype(jnp.bfloat16), "tp", scatter_dimension=0, tiled=True
    ).astype(jnp.float32)
    branch = normalize(head_sum, attn_gain)
    kept = (residual_in.astype(jnp.float32) + branch).astype(jnp.bfloat16)
    normed = normalize(kept.astype(jnp.float32), mlp_gain).astype(jnp.bfloat16)
    whole_normed = lax.all_gather(normed, "tp", axis=0, tiled=True)
    gate_whole, up_whole, down_whole = (
        lax.all_gather(gate_weight, "sp", axis=0, tiled=True),
        lax.all_gather(up_weight, "sp", axis=0, tiled=True),
        lax.all_gather(down_weight, "sp", axis=1, tiled=True),
    )
    gate = jnp.dot(whole_normed, gate_whole, preferred_element_type=jnp.float32)
    up = jnp.dot(whole_normed, up_whole, preferred_element_type=jnp.float32)
    hidden = (jax.nn.silu(gate) * up).astype(jnp.bfloat16)
    rows = hidden
    channel_sum = lax.psum_scatter(
        jnp.dot(rows, down_whole, preferred_element_type=jnp.float32).astype(jnp.bfloat16),
        "tp",
        scatter_dimension=0,
        tiled=True,
    ).astype(jnp.float32)
    return (kept.astype(jnp.float32) + 0.5 * channel_sum).astype(jnp.bfloat16)


LOG2E = math.log2(math.e)


def grid_of(mesh):
    n_sp, n_tp = mesh.shape["sp"], mesh.shape["tp"]
    devices = mesh.devices.reshape(n_sp, n_tp)
    try:
        places = [tuple(device.coords) for device in devices[:, 0]]
        partners = [tuple(device.coords) for device in devices[:, -1]]
    except Exception:
        return (n_sp // 4, 2, 2) if n_sp % 4 == 0 else None
    if places != partners:
        return None
    low = [min(place[k] for place in places) for k in range(3)]
    sizes = [max(place[k] for place in places) - low[k] + 1 for k in range(3)]
    wide_z, wide_y, wide_x = sizes[2], sizes[1], sizes[0]
    if wide_z * wide_y * wide_x != n_sp:
        return None
    for index, place in enumerate(places):
        x, y, z = (place[k] - low[k] for k in range(3))
        if (z * wide_y + y) * wide_x + x != index:
            return None
    return wide_z, wide_y, wide_x


def hop_table(grid):
    wide_z = grid[0]
    entries = [
        (dz, fy, fx)
        for dz in range(1 - wide_z, wide_z)
        for fy in range(2)
        for fx in range(2)
        if (dz, fy, fx) != (0, 0, 0)
    ]
    entries.sort(key=lambda e: (abs(e[0]) + e[1] + e[2], abs(e[0]), e))
    return entries


def layer_kernel(
    grid, shapes, res_in, qlt, qbt, lat_in, rope_in, lg, ag, mg, kul, kub_in, vul, vub_in, wol_in, wob_in, gw, uw, dw, out,
    lat, kub, vub, cosine, sine, lat_all, gate_all, up_all, down_all, ext_all, own_g, own_u, own_d, own_e, ql, qb, keyn, scores, weigh, valt_l, valt_b,
    peak, total, acc_l, acc_b, att, term, inbox, kept, rows_all, hidden, inbox2, psum, inbox3, wol, wob, res,
    lat_recv, lat_send, lat_pair, recv, send, own_sem, pair_send, pair_recv,
):
    wide_z, wide_y, wide_x = grid
    n_sp = wide_z * wide_y * wide_x
    tokens, share, rope = shapes
    heads_l, heads_b = qlt.shape[0], qbt.shape[0]
    bf16, f32 = jnp.bfloat16, jnp.float32
    me = lax.axis_index("sp")
    core = lax.axis_index("tp")
    my_x = lax.rem(me, wide_x)
    my_y = lax.rem(me // wide_x, wide_y)
    my_z = me // (wide_x * wide_y)
    layer = wide_y * wide_x
    flip_y = me + (1 - 2 * my_y) * wide_x
    flip_x = me + (1 - 2 * my_x)
    side = lax.rem(my_z, 2)
    partner = me + (1 - 2 * side) * layer
    z_ways = [
        (step, my_z + step < wide_z if step > 0 else my_z + step >= 0,
         jnp.clip(me + step * layer, 0, n_sp - 1))
        for step in (1, -1, 2, -2, 3, -3)
    ]

    def z_way(step):
        return next(way for way in z_ways if way[0] == step)

    def run(condition, action):
        pl.when(condition)(action)

    gate_rows, units = gw.shape
    down_cols = dw.shape[1]
    extra = ext_all.shape[2]
    main = (units - extra) // 2
    fetch = [
        pltpu.make_async_copy(src, dst, own_sem.at[k])
        for k, (src, dst) in enumerate((
            (gw, own_g), (uw, own_u), (dw, own_d),
            (gw.at[:, pl.ds(2 * main, extra)], own_e.at[0]),
            (uw.at[:, pl.ds(2 * main, extra)], own_e.at[1]),
            (dw.at[pl.ds(2 * main, extra), :], own_e.at[2]),
            (wol_in, wol), (wob_in, wob), (res_in, res),
        ))
    ]
    for copy in fetch:
        copy.start()
    half_rope = rope // 2
    lane = lax.broadcasted_iota(jnp.int32, (half_rope, tokens), 1)
    line = lax.broadcasted_iota(jnp.int32, (half_rope, tokens), 0)
    freqs = jnp.zeros((half_rope, tokens), f32)
    for k in range(half_rope):
        freqs = jnp.where(line == k, THETA ** (-2.0 * k / rope), freqs)
    angle = (me * tokens + lane).astype(f32) * freqs
    cosine[...] = jnp.cos(angle)
    sine[...] = jnp.sin(angle)
    lat[:tokens, :] = normalize(lat_in[...].astype(f32), lg[...]).astype(bf16)
    one, two = rope_in[:half_rope, :].astype(f32), rope_in[half_rope:, :].astype(f32)
    lat[tokens:tokens + half_rope, :] = (one * cosine[...] - two * sine[...]).astype(bf16)
    lat[tokens + half_rope:, :] = (one * sine[...] + two * cosine[...]).astype(bf16)
    lat_rows = lat.shape[0]
    barrier = pltpu.get_barrier_semaphore()
    for where in (flip_x, flip_y):
        pl.semaphore_signal(barrier, inc=1, device_id={"sp": where})
    pl.semaphore_signal(barrier, inc=1, device_id={"tp": 1 - core})
    greeted = 3
    for _, exists, where in z_ways:
        run(exists, lambda where=where: pl.semaphore_signal(barrier, inc=1, device_id={"sp": where}))
        greeted = greeted + jnp.where(exists, 1, 0)
    pl.semaphore_wait(barrier, greeted)

    half = lat_rows // 2
    first = pl.multiple_of(core * half, 16)

    def lat_at(i):
        return lat_all.at[pl.ds(pl.multiple_of(i * lat_rows + first, 16), half)]

    def lat_copy(i, mine, where):
        return pltpu.make_async_remote_copy(
            src_ref=lat.at[pl.ds(first, half)] if mine else lat_at(i), dst_ref=lat_at(i),
            send_sem=lat_send.at[0], recv_sem=lat_recv.at[i], device_id={"sp": where},
        )

    def pair_lat(i):
        return pltpu.make_async_remote_copy(
            src_ref=lat_at(i), dst_ref=lat_at(i), send_sem=lat_send.at[1],
            recv_sem=lat_pair.at[i], device_id={"tp": 1 - core},
        )

    turn = jnp.where(core == 0, flip_x, flip_y)
    away = jnp.where(core == 0, flip_y, flip_x)

    def lat_spread(i, mine):
        _, exists, where = z_way(1)
        run(exists, lambda: lat_copy(i, mine, where).start())
        lat_copy(i, mine, turn).start()
        lat_copy(i, mine, away).start()

    lat_spread(me, True)

    per = 4

    def words_of(table):
        codes = [((dz + wide_z - 1) * 2 + fy) * 2 + fx for dz, fy, fx in table]
        return [
            sum(code << (7 * k) for k, code in enumerate(codes[at:at + per]))
            for at in range(0, len(codes), per)
        ]

    def origin_of(n, words):
        word = jnp.int32(words[0])
        for k in range(1, len(words)):
            word = jnp.where(n // per == k, jnp.int32(words[k]), word)
        rem = lax.rem(n, per)
        for k in range(1, per):
            word = jnp.where(rem >= k, word // 128, word)
        code = lax.rem(word, 128)
        return code // 4 - (wide_z - 1), lax.rem(code // 2, 2), lax.rem(code, 2)

    def index_of(dz, fy, fx):
        oy = my_y + fy * (1 - 2 * my_y)
        ox = my_x + fx * (1 - 2 * my_x)
        return ((my_z + dz) * wide_y + oy) * wide_x + ox

    def lat_event(dz, fy, fx, column, line):
        i = index_of(dz, fy, fx)
        lat_copy(i, False, turn).wait_recv()
        if column:
            lat_spread(i, False)
        if line:
            lat_copy(i, False, away).start()
        pair_lat(i).start()

    def lat_column(down):
        run(my_z >= down, lambda: lat_event(-down, 0, 0, True, False))

    def lat_side(down):
        def events_of():
            near = jnp.where(core == 0, 0, 1)
            lat_event(-down, near, 1 - near, False, True)
            lat_event(-down, 1 - near, near, False, False)

        run(my_z >= down, events_of)

    def lat_far(down):
        run(my_z >= down, lambda: lat_event(-down, 1, 1, False, False))

    def slot_at(ref, i):
        return ref.at[pl.ds(pl.multiple_of(i * gate_rows, gate_rows), gate_rows), pl.ds(0, main)]

    def down_slot(dz, fy, fx):
        slot = (fy * 2 + fx) * wide_z + my_z + dz
        return down_all.at[pl.ds(0, main), pl.ds(pl.multiple_of(slot * down_cols, down_cols), down_cols)]

    def place(p, dz, fy, fx):
        i = index_of(dz, fy, fx)
        if p == 0:
            return slot_at(gate_all, i)
        if p == 1:
            return slot_at(up_all, i)
        if p == 2:
            return down_slot(dz, fy, fx)
        return ext_all.at[i]

    def own_half(p, h):
        lanes = pl.ds(pl.multiple_of(h * main, extra), main)
        if p == 0:
            return own_g.at[:, lanes]
        if p == 1:
            return own_u.at[:, lanes]
        if p == 2:
            return own_d.at[lanes, :]
        return own_e

    def part_copy(p, src, dst, i, where):
        return pltpu.make_async_remote_copy(
            src_ref=src, dst_ref=dst, send_sem=send.at[p], recv_sem=recv.at[p, i], device_id={"sp": where},
        )

    has_extra = core == side

    def to_z(p, src, step, origin, i, condition=True):
        _, exists, where = z_way(step)
        dst = place(p, *origin) if p == 2 else place(p, *origin)
        run(jnp.logical_and(exists, condition), lambda: part_copy(p, src, dst, i, where).start())

    def seen(origin, fy, fx):
        return origin[0], origin[1] + fy - 2 * origin[1] * fy, origin[2] + fx - 2 * origin[2] * fx

    def dst_for(p, origin, fy, fx):
        if p == 2:
            return down_slot(*seen(origin, fy, fx))
        return place(p, *origin)

    def send_own(p, steps, in_layer, when=True):
        here = (0, 0, 0)
        mine = own_half(p, side)
        other = own_half(p, 1 - side)
        same = has_extra if p == 3 else True
        cross = jnp.logical_not(has_extra) if p == 3 else True
        for step in steps:
            if step % 2:
                to_z(p, other, step, here, me, jnp.logical_and(cross, when))
            else:
                to_z(p, mine, step, here, me, jnp.logical_and(same, when))

        def flips():
            part_copy(p, mine, dst_for(p, here, 0, 1), me, flip_x).start()
            part_copy(p, mine, dst_for(p, here, 1, 0), me, flip_y).start()

        if in_layer:
            run(jnp.logical_and(same, when), flips)

    def part_event(p, dz, fy, fx):
        origin = (dz, fy, fx)
        i = index_of(*origin)
        here = place(p, *origin)
        part_copy(p, here, here, i, flip_x).wait_recv()
        column = jnp.logical_and(fy == 0, fx == 0)
        x_line = jnp.logical_and(fy == 0, fx == 1)
        y_line = jnp.logical_and(fy == 1, fx == 0)
        if p == 0:
            to_x, to_y = column, jnp.logical_or(column, x_line)
        elif p == 1:
            to_x, to_y = jnp.logical_or(column, y_line), column
        else:
            x_first = core == 0 if p == 2 else lax.rem(my_z + dz, 2) == 0
            to_x = jnp.logical_or(column, jnp.logical_and(y_line, jnp.logical_not(x_first)))
            to_y = jnp.logical_or(column, jnp.logical_and(x_line, x_first))
        run(to_x, lambda: part_copy(p, here, dst_for(p, origin, 0, 1), i, flip_x).start())
        run(to_y, lambda: part_copy(p, here, dst_for(p, origin, 1, 0), i, flip_y).start())

    for copy in fetch[:6]:
        copy.wait()
    gates = (0, 1, 3, 2)
    for p in gates:
        send_own(p, (-1, -2, -3), False)
        send_own(p, (1, 2, 3), False, my_z == 0)
    lat_column(1)
    for p in gates:
        send_own(p, (1, 2, 3), False, my_z == 1)
    lat_side(0)
    for p in gates[:2]:
        send_own(p, (), True, my_z == 2)
    if wide_z > 2:
        lat_column(2)
        for p in gates:
            send_own(p, (1, 2, 3), False, my_z == 2)
    lat_side(1)
    for p in gates[:2]:
        send_own(p, (), True, my_z != 2)
    for p in gates[2:]:
        send_own(p, (), True)
    lat_far(0)
    lat_far(1)

    whole = hop_table(grid)
    whole_words = words_of(whole)
    count = len(whole)
    hops = [abs(dz) + fy + fx for dz, fy, fx in whole]
    early = sum(1 for hop in hops if hop <= 2)
    ready = sum(1 for hop in hops if hop < wide_z)
    early = sum(1 for hop in hops if hop <= 2)
    groups = ((0, 0), (0, 1), (1, 0), (1, 1))
    grouped = whole
    grouped_words = words_of(grouped)
    lag = count - ready

    def inside(dz):
        return jnp.logical_and(my_z + dz >= 0, my_z + dz < wide_z)

    def events(low, high):
        def gate_parts(n):
            dz, fy, fx = origin_of(n, whole_words)

            @pl.when(inside(dz))
            def _():
                part_event(0, dz, fy, fx)
                part_event(1, dz, fy, fx)
                run(has_extra, lambda: part_event(3, dz, fy, fx))

        def downs(n):
            dz, fy, fx = origin_of(n, grouped_words)
            run(inside(dz), lambda: part_event(2, dz, fy, fx))

        def body(t, _):
            run(t < count, lambda: gate_parts(t))
            run(t >= lag, lambda: downs(t - lag))
            return 0

        lax.fori_loop(low, high, body, 0)

    own_rows = pl.ds(pl.multiple_of(me * gate_rows, gate_rows), gate_rows)
    own_lanes = pl.ds(pl.multiple_of(side * main, extra), main)
    gate_all[own_rows, :main] = own_g[:, own_lanes]
    up_all[own_rows, :main] = own_u[:, own_lanes]
    down_all[:main, pl.ds(pl.multiple_of(my_z * down_cols, down_cols), down_cols)] = own_d[own_lanes, :]
    ext_all[me] = own_e[...]

    wide_l = kul.shape[0] // heads_l
    wide_b = kub.shape[1] // heads_b
    for h in range(heads_b):
        part = slice(h * wide_b, (h + 1) * wide_b)
        kub[:, part] = kub_in[:, h, :]
        vub[part, :] = vub_in[:, h, :].T
    for given, query in ((qlt, ql), (qbt, qb)):
        nope = given.shape[1] - rope
        for h in range(given.shape[0]):
            one = given[h, nope:nope + half_rope, :].astype(f32)
            two = given[h, nope + half_rope:, :].astype(f32)
            if nope < wide_b:
                query[h, :wide_b, :] = jnp.zeros((wide_b, tokens), bf16)
            at = (h * nope) % wide_b
            query[h, at:at + nope, :] = given[h, :nope, :]
            query[h, wide_b:wide_b + half_rope, :] = (one * cosine[...] - two * sine[...]).astype(bf16)
            query[h, wide_b + half_rope:, :] = (one * sine[...] + two * cosine[...]).astype(bf16)
    lat_all[pl.ds(pl.multiple_of(me * lat_rows, 16), lat_rows), :] = lat[...]

    peak[...] = jnp.full(peak.shape, NEGATIVE, f32)
    total[...] = jnp.zeros(total.shape, f32)
    acc_l[...] = jnp.zeros(acc_l.shape, f32)
    acc_b[...] = jnp.zeros(acc_b.shape, f32)
    contract = (((1,), (1,)), ((), ()))
    strip = math.gcd(tokens, 64)
    strips = [slice(at, at + strip) for at in range(0, tokens, strip)]

    def attend_block(j, masked):
        at_j = pl.multiple_of(j * lat_rows, 16)
        rows = lat_all[pl.ds(at_j, tokens), :]
        rot = lat_all[pl.ds(pl.multiple_of(at_j + tokens, 16), rope), :].T
        split = heads_l * wide_l
        keyn[:, :split] = lax.dot_general(rows, kul[...], contract, preferred_element_type=f32).astype(bf16)
        keyn[:, split:] = jnp.dot(rows, kub[...], preferred_element_type=f32).astype(bf16)
        for ups, held in ((vul, valt_l), (vub, valt_b)):
            held[...] = lax.dot_general(
                ups[...], rows, contract, preferred_element_type=f32
            ).astype(bf16)

        def of(g):
            if g < heads_l:
                return g, ql, valt_l, acc_l, wide_l, wide_l + rope
            return g - heads_l, qb, valt_b, acc_b, wide_b, wide_b + rope

        def score(g):
            h, query = of(g)[:2]
            at = (g * wide_l // wide_b if g < heads_l else split // wide_b + h) * wide_b
            keys = jnp.concatenate([keyn[:, at:at + wide_b], rot], axis=1)
            held = jnp.dot(keys, query[h], preferred_element_type=f32)
            if masked:
                key_pos = lax.broadcasted_iota(jnp.int32, (tokens, tokens), 0)
                visible = key_pos <= lax.broadcasted_iota(jnp.int32, (tokens, tokens), 1)
                held = jnp.where(visible, held, NEGATIVE)
            scores[g % 2] = held

        score(0)
        for g in range(heads_l + heads_b):
            if g + 1 < heads_l + heads_b:
                score(g + 1)
            h, query, held, acc, wide, size = of(g)
            scale = LOG2E * size ** (-0.5)
            old = peak[g]
            top = jnp.max(scores[g % 2, strips[0], :], axis=0, keepdims=True)
            for part in strips[1:]:
                top = jnp.maximum(top, jnp.max(scores[g % 2, part, :], axis=0, keepdims=True))
            new = jnp.maximum(old, top * scale)
            factor = jnp.exp2(old - new)
            summed = total[g] * factor
            for part in strips:
                weights = jnp.exp2(scores[g % 2, part, :] * scale - new)
                summed = summed + jnp.sum(weights, axis=0, keepdims=True)
                weigh[g % 2, part, :] = weights.astype(bf16)
            peak[g] = new
            total[g] = summed
            acc[h] = acc[h] * factor + jnp.dot(
                held[h * wide:(h + 1) * wide, :], weigh[g % 2], preferred_element_type=f32
            )

    def attend_layer(down, low, high):
        def body(t, _):
            events(low + (t * (high - low)) // layer, low + ((t + 1) * (high - low)) // layer)
            i = (my_z - down) * layer + t

            @pl.when(jnp.logical_and(my_z >= down, i < me))
            def _():
                pair_lat(i).wait_recv()
                attend_block(i, False)

            return 0

        lax.fori_loop(0, layer, body, 0)

    attend_block(me, True)
    attend_layer(0, 0, 0)
    for down in range(1, wide_z):
        if down == 1 and wide_z > 2:
            lat_column(3)
            lat_side(2)
            lat_far(2)
        if down == 2:
            lat_side(3)
            lat_far(3)
        attend_layer(down, (down - 1) * early // (wide_z - 1), down * early // (wide_z - 1))

    def rest(i, _):
        run(jnp.logical_and(i > me, i < (my_z + 1) * layer), lambda: pair_lat(i).wait_recv())
        return 0

    lax.fori_loop(0, n_sp, rest, 0)

    split = heads_l * wide_l
    for heads, wide, acc, base, col in (
        (heads_l, wide_l, acc_l, 0, 0), (heads_b, wide_b, acc_b, heads_l, split),
    ):
        together = wide_b // wide
        for h in range(0, heads, together):
            done = jnp.concatenate(
                [acc[h + k] / total[base + h + k] for k in range(together)], axis=0
            )
            att[:, col + h * wide:col + (h + together) * wide] = done.T.astype(bf16)

    features = out.shape[1]
    block = math.gcd(features, 512)

    for copy in fetch[6:]:
        copy.wait()

    def project(n, _):
        cols = pl.ds(pl.multiple_of(n * block, block), block)
        term[:tokens, cols] = (
            jnp.dot(att[:, :split], wol[:, cols], preferred_element_type=f32)
            + jnp.dot(att[:, split:], wob[:, cols], preferred_element_type=f32)
        ).astype(bf16)
        return 0

    lax.fori_loop(0, features // block, project, 0)
    theirs = pl.ds(pl.multiple_of((1 - core) * share, share), share)

    def to_pair(k, src, dst):
        return pltpu.make_async_remote_copy(
            src_ref=src, dst_ref=dst, send_sem=pair_send.at[k], recv_sem=pair_recv.at[k],
            device_id={"tp": 1 - core},
        )

    def to_partner(k, src, dst):
        return pltpu.make_async_remote_copy(
            src_ref=src, dst_ref=dst, send_sem=pair_send.at[k], recv_sem=pair_recv.at[k],
            device_id={"sp": partner},
        )

    def place_of(of_core, of_side):
        return pl.ds(pl.multiple_of((of_side * 2 + of_core) * share, share), share)

    heads_out = to_pair(0, term.at[theirs], inbox)
    heads_out.start()
    heads_out.wait_recv()
    rows_at_once = math.gcd(share, 16)

    def norms(n, _):
        rows = pl.ds(pl.multiple_of(n * rows_at_once, rows_at_once), rows_at_once)
        full = pl.ds(pl.multiple_of(core * share + n * rows_at_once, rows_at_once), rows_at_once)
        spot = pl.ds(pl.multiple_of((side * 2 + core) * share + n * rows_at_once, rows_at_once), rows_at_once)
        summed = term[full, :].astype(f32) + inbox[rows, :].astype(f32)
        branch = normalize(summed, ag[...])
        mixed = (res[rows, :].astype(f32) + branch).astype(bf16)
        kept[rows, :] = mixed
        rows_all[spot, :] = normalize(mixed.astype(f32), mg[...]).astype(bf16)
        return 0

    lax.fori_loop(0, share // rows_at_once, norms, 0)
    mine_at = rows_all.at[place_of(core, side)]
    rows_out = to_pair(1, mine_at, mine_at)
    rows_far = to_partner(2, mine_at, mine_at)
    rows_out.start()
    rows_far.start()
    heads_out.wait_send()
    ready = sum(1 for hop in hops if hop < wide_z)
    events(early, ready)
    far_at = rows_all.at[place_of(core, 1 - side)]
    to_partner(2, far_at, far_at).wait_recv()
    rows_on = to_pair(3, far_at, far_at)
    rows_on.start()
    near_at = rows_all.at[place_of(1 - core, side)]
    to_pair(1, near_at, near_at).wait_recv()
    last_at = rows_all.at[place_of(1 - core, 1 - side)]
    to_pair(3, last_at, last_at).wait_recv()
    events(ready, count)

    def feed_from(rows, gate_w, up_w, cols):
        gate = jnp.dot(rows_all[rows, :], gate_w, preferred_element_type=f32)
        up = jnp.dot(rows_all[rows, :], up_w, preferred_element_type=f32)
        hidden[rows, cols] = (gate / (1.0 + jnp.exp(-gate)) * up).astype(bf16)

    span = 256
    chunks = main // span
    group = tokens

    def group_rows(n):
        of_side = jnp.where(n == 0, 1 - side, side)
        return pl.ds(pl.multiple_of(of_side * group, group), group)

    @pl.when(has_extra)
    def _():
        def lay(i, _):
            oz = i // layer
            fy = jnp.abs(lax.rem(i // wide_x, wide_y) - my_y)
            fx = jnp.abs(lax.rem(i, wide_x) - my_x)
            slot = (fy * 2 + fx) * wide_z + oz
            at_i = pl.ds(pl.multiple_of(i * gate_rows, gate_rows), gate_rows)
            gate_all[at_i, main:] = ext_all[i, 0]
            up_all[at_i, main:] = ext_all[i, 1]
            down_all[main:, pl.ds(pl.multiple_of(slot * down_cols, down_cols), down_cols)] = ext_all[i, 2]
            return 0

        lax.fori_loop(0, n_sp, lay, 0)

    def feed(half):
        rows = group_rows(half)

        def body(n, _):
            cols = pl.ds(pl.multiple_of(n * span, span), span)
            feed_from(rows, gate_all[:, cols], up_all[:, cols], cols)
            return 0

        lax.fori_loop(0, chunks, body, 0)

        def rest(high):
            cols = slice(chunks * span, high)
            if high > chunks * span:
                feed_from(rows, gate_all[:, cols], up_all[:, cols], cols)

        run(has_extra, lambda: rest(main + extra))
        run(jnp.logical_not(has_extra), lambda: rest(main))

    wide_k = wide_z * down_cols
    wide_n = math.gcd(wide_k, 256)
    pieces = wide_k // wide_n

    def down_with(depth, half, low, high):
        rows = group_rows(half)

        def body(n, _):
            cols = pl.ds(pl.multiple_of(n * wide_n, wide_n), wide_n)
            term[rows, cols] = jnp.dot(
                hidden[rows, :depth], down_all[:depth, cols], preferred_element_type=f32
            ).astype(bf16)
            return 0

        lax.fori_loop(low * pieces, high * pieces, body, 0)

    def down(half, low, high):
        run(has_extra, lambda: down_with(main + extra, half, low, high))
        run(jnp.logical_not(has_extra), lambda: down_with(main, half, low, high))

    sums, sums_far = [], []

    def pair_sums(k):
        cols = pl.ds(k * wide_k, wide_k)
        sums.append(to_pair(4 + k, term.at[place_of(1 - core, 1 - side), cols], inbox2.at[pl.ds(0, share), cols]))
        sums[k].start()

    def far_sums(k):
        cols = pl.ds(k * wide_k, wide_k)
        sums[k].wait_recv()
        psum[:, cols] = (
            term[place_of(core, 1 - side), cols].astype(f32) + inbox2[:share, cols].astype(f32)
        ).astype(bf16)
        sums_far.append(to_partner(8 + k, psum.at[:, cols], inbox3.at[:, cols]))
        sums_far[k].start()

    feed(0)
    since = count
    for k, (fy, fx) in enumerate(groups):
        until = lag + max(n + 1 for n, e in enumerate(grouped) if e[1:] == (fy, fx))
        until = max(until, since)
        events(max(since, count), max(until, count))
        since = until
        down(0, k, k + 1)
        pair_sums(k)
        if k:
            far_sums(k - 1)
    far_sums(len(groups) - 1)
    feed(1)
    down(1, 0, len(groups))
    own_sums = to_pair(12, term.at[place_of(1 - core, side)], inbox2.at[pl.ds(share, share)])
    own_sums.start()

    def drain(ref, sem):
        pltpu.make_async_copy(ref, ref, sem).wait()

    for z in range(wide_z):
        @pl.when(my_z == z)
        def _(z=z):
            up = 1 if z + 1 < wide_z else 0
            drain(lat_all.at[pl.ds(0, (up + 3) * (z + 1) * half)], lat_send.at[0])
            drain(lat_all.at[pl.ds(0, (layer * (z + 1) - 1) * half)], lat_send.at[1])
            two = (1 if z + 2 < wide_z else 0) + (1 if z >= 2 else 0)
            odd = sum(1 for step in (1, -1, 3, -3) if 0 <= z + step < wide_z)
            n = two + odd + 3 * wide_z
            drain(gate_all.at[pl.ds(0, n * gate_rows), pl.ds(0, main)], send.at[0])
            drain(up_all.at[pl.ds(0, n * gate_rows), pl.ds(0, main)], send.at[1])
            drain(down_all.at[pl.ds(0, main), pl.ds(0, n * down_cols)], send.at[2])
            run(has_extra, lambda: drain(ext_all.at[pl.ds(0, two + 3 * wide_z)], send.at[3]))
            run(jnp.logical_not(has_extra), lambda: drain(ext_all.at[pl.ds(0, odd)], send.at[3]))

    own_sums.wait_recv()
    for copy in [rows_out, rows_far, rows_on, own_sums] + sums:
        copy.wait_send()

    for k, (fy, fx) in enumerate(groups):
        sums_far[k].wait_recv()

        def finish(t, _, k=k, fy=fy, fx=fx):
            slot = pl.ds(pl.multiple_of((k * wide_z + t) * down_cols, down_cols), down_cols)
            i = (t * wide_y + my_y + fy * (1 - 2 * my_y)) * wide_x + my_x + fx * (1 - 2 * my_x)
            cols = pl.ds(pl.multiple_of(i * down_cols, down_cols), down_cols)
            summed = (
                term[place_of(core, side), slot].astype(f32)
                + inbox2[share:, slot].astype(f32)
                + inbox3[:, slot].astype(f32)
            )
            out[:, cols] = (kept[:, cols].astype(f32) + 0.5 * summed).astype(bf16)
            return 0

        lax.fori_loop(0, wide_z, finish, 0)
    for copy in sums_far:
        copy.wait_send()


def fused_shards(
    grid, residual_in, query_lean, query_broad, latent, rope_key, latent_gain, key_up_lean,
    key_up_broad, value_up_lean, value_up_broad, out_lean, out_broad, attn_gain, mlp_gain,
    gate_weight, up_weight, down_weight,
):
    bf16, f32 = jnp.bfloat16, jnp.float32
    tokens = query_lean.shape[0]
    share, features = residual_in.shape
    rank = latent.shape[1]
    rope = rope_key.shape[1]
    n_sp = lax.axis_size("sp")
    ql, qb = (jnp.transpose(query, (1, 2, 0)) for query in (query_lean, query_broad))
    kul = key_up_lean.reshape(rank, -1).T
    vul = value_up_lean.reshape(rank, -1).T
    wol = out_lean.reshape(-1, features)
    wob = out_broad.reshape(-1, features)
    heads = ql.shape[0] + qb.shape[0]
    wide_all = qb.shape[0] * value_up_broad.shape[2]
    units = gate_weight.shape[1]
    extra = gate_weight.shape[0]
    main = (units - extra) // 2
    wide_b = value_up_broad.shape[2]
    vmem = pl.BlockSpec(memory_space=pltpu.VMEM)
    args = (
        residual_in, ql, qb, latent, rope_key.T, latent_gain[None], attn_gain[None], mlp_gain[None],
        kul, key_up_broad, vul, value_up_broad, wol, wob,
        gate_weight, up_weight, down_weight,
    )
    dma = pltpu.SemaphoreType.DMA
    return pl.pallas_call(
        functools.partial(layer_kernel, grid, (tokens, share, rope)),
        out_shape=jax.ShapeDtypeStruct((share, features), bf16),
        in_specs=[
            pl.BlockSpec(memory_space=pl.ANY) if k in (0, 12, 13, 14, 15, 16) else vmem for k in range(len(args))
        ],
        out_specs=vmem,
        scratch_shapes=[
            pltpu.VMEM((tokens + rope, rank), bf16),
            pltpu.VMEM((rank, wide_all), bf16),
            pltpu.VMEM((wide_all, rank), bf16),
            pltpu.VMEM((rope // 2, tokens), f32),
            pltpu.VMEM((rope // 2, tokens), f32),
            pltpu.VMEM((n_sp * (tokens + rope), rank), bf16),
            pltpu.VMEM((features, main + extra), bf16),
            pltpu.VMEM((features, main + extra), bf16),
            pltpu.VMEM((main + extra, features), bf16),
            pltpu.VMEM((n_sp, 3, extra, extra), bf16),
            pltpu.VMEM(gate_weight.shape, bf16),
            pltpu.VMEM(up_weight.shape, bf16),
            pltpu.VMEM(down_weight.shape, bf16),
            pltpu.VMEM((3, extra, extra), bf16),
            pltpu.VMEM((ql.shape[0],) + qb.shape[1:], bf16),
            pltpu.VMEM(qb.shape, bf16),
            pltpu.VMEM((tokens, kul.shape[0] + wide_all), bf16),
            pltpu.VMEM((2, tokens, tokens), f32),
            pltpu.VMEM((2, tokens, tokens), bf16),
            pltpu.VMEM((vul.shape[0], tokens), bf16),
            pltpu.VMEM((wide_all, tokens), bf16),
            pltpu.VMEM((heads, 1, tokens), f32),
            pltpu.VMEM((heads, 1, tokens), f32),
            pltpu.VMEM((ql.shape[0], value_up_lean.shape[2], tokens), f32),
            pltpu.VMEM((qb.shape[0], wide_b, tokens), f32),
            pltpu.VMEM((tokens, vul.shape[0] + wide_all), bf16),
            pltpu.VMEM((2 * tokens, features), bf16),
            pltpu.VMEM((share, features), bf16),
            pltpu.VMEM((share, features), bf16),
            pltpu.VMEM((2 * tokens, features), bf16),
            pltpu.VMEM((2 * tokens, main + extra), bf16),
            pltpu.VMEM((2 * share, features), bf16),
            pltpu.VMEM((share, features), bf16),
            pltpu.VMEM((share, features), bf16),
            pltpu.VMEM(wol.shape, bf16),
            pltpu.VMEM(wob.shape, bf16),
            pltpu.VMEM(residual_in.shape, bf16),
            dma((n_sp,)),
            dma((2,)),
            dma((n_sp,)),
            dma((4, n_sp)),
            dma((4,)),
            dma((10,)),
            dma((13,)),
            dma((13,)),
        ],
        compiler_params=pltpu.CompilerParams(
            collective_id=0, has_side_effects=True, vmem_limit_bytes=62 * 2**20
        ),
    )(*args)


def fits(grid, mesh, args):
    if grid is None or mesh.shape["tp"] != 2 or grid[1] != 2 or grid[2] != 2 or grid[0] not in (2, 4, 6, 8):
        return False
    n_sp = mesh.shape["sp"]
    tokens = args[1].shape[0] // n_sp
    share = tokens // 2
    units = args[14].shape[1] // 2
    heads_l, heads_b = args[6].shape[1] // 2, args[7].shape[1] // 2
    wide_l, wide_b = args[6].shape[2], args[7].shape[2]
    rope = args[4].shape[1]
    return (
        tokens % 128 == 0 and tokens <= 256 and share % 16 == 0 and units >= 384
        and units % 256 == 128 and heads_l % 2 == 0 and 2 * wide_l == wide_b and wide_b % 128 == 0
        and args[3].shape[1] == tokens and rope % 32 == 0 and (tokens + rope) % 32 == 0
        and heads_b > 0 and args[8].shape[2] == wide_l and args[9].shape[2] == wide_b
        and args[14].shape[0] // n_sp == 128 and args[16].shape[1] // n_sp == 128
    )


def solution(mesh):
    in_specs = (
        P(("sp", "tp"), None),
        P("sp", "tp", None),
        P("sp", "tp", None),
        P("sp", None),
        P("sp", None),
        P(),
        P(None, "tp", None),
        P(None, "tp", None),
        P(None, "tp", None),
        P(None, "tp", None),
        P("tp", None, None),
        P("tp", None, None),
        P(),
        P(),
        P("sp", "tp"),
        P("sp", "tp"),
        P("tp", "sp"),
    )
    out_specs = P(("sp", "tp"), None)
    grid = grid_of(mesh)

    def layer(*args):
        body = functools.partial(fused_shards, grid) if fits(grid, mesh, args) else shards
        return jax.shard_map(
            body, mesh=mesh, in_specs=in_specs, out_specs=out_specs, check_vma=False
        )(*args)

    return layer
```
